32 devices in a mesh: rep: 2 (over x), fs: 8 (over z, y), tp: 2 (over core).
Axes of the slice: x: 2, y: 2, z: 4, core: 2. Of those that a mesh axis runs over, the one named last changes fastest.
Arguments:
- tokens: bfloat16 [8192, 2048], P(('rep', 'fs')), may hold values from -3 to 3
- mixer_gain: float32 [2048], replicated, may hold values from 0.1 to 1.9
- mix_weight: bfloat16 [2048, 1024], P('fs', 'tp'), may hold values from -0.125 to 0.125
- mixer_conv: float32 [4, 1024], P(None, 'tp'), may hold values from -3 to 3
- mixer_offset: float32 [1024], P('tp'), may hold values from -0.06 to 0.06
- recur_weight: bfloat16 [8, 128, 128], P('tp'), may hold values from -0.5 to 0.5
- recur_bias: float32 [1024], P('tp'), may hold values from -3 to 3
- input_weight: bfloat16 [8, 128, 128], P('tp'), may hold values from -0.5 to 0.5
- input_bias: float32 [1024], P('tp'), may hold values from 1 to 3
- decay_logit: float32 [1024], P('tp'), may hold values from 4 to 11
- out_weight: bfloat16 [1024, 2048], P('tp', 'fs'), may hold values from -0.375 to 0.375
- channel_gain: float32 [2048], replicated, may hold values from 0.1 to 1.9
- gate_weight: bfloat16 [2048, 6144], P('fs', 'tp'), may hold values from -0.125 to 0.125
- up_weight: bfloat16 [2048, 6144], P('fs', 'tp'), may hold values from -0.125 to 0.125
- gate_conv: float32 [3, 6144], P(None, 'tp'), may hold values from -3.5 to 3.5
- gate_offset: float32 [6144], P('tp'), may hold values from -3 to 3
- down_weight: bfloat16 [6144, 2048], P('tp', 'fs'), may hold values from -0.078125 to 0.078125
Outputs:
- layer_out: bfloat16 [8192, 2048], P(('rep', 'fs'))
The draws below stay inside these ranges and needn't reach their ends.
All inputs are finite; a program needn't handle non-finite values.
Results may differ from the reference program's by a relative error of at most 0.023.
Values may be sent and summed in bfloat16 or wider, within the bound.
A program may use at most 128 MiB of HBM per device.

```python
import jax
import jax.numpy as jnp
from jax import lax

D = 2048
LRU = 1024
BLOCKS = 8
BLOCK_DIM = 128
MIX_TAPS = 4
FF = 6144
MLP_TAPS = 3
SEQLEN = 512
SEQS = 16
TOKENS = 8192
N_TP = 2


def draw_decay_logit(key, part):
    pick_key = jax.random.fold_in(key, 11)
    slow_key = jax.random.fold_in(key, 12)
    fast_key = jax.random.fold_in(key, 13)
    fast_share = 0.5
    fast = jax.random.bernoulli(pick_key, fast_share, (LRU,))
    slow_rate = jax.random.uniform(slow_key, (LRU,), jnp.float32, 1.0, 2.3) / SEQLEN
    fast_rate = jax.random.uniform(fast_key, (LRU,), jnp.float32, 0.02, 0.08)
    rate = jnp.where(fast, fast_rate, slow_rate) / 8.0
    return -rate - jnp.log(-jnp.expm1(-rate))


def steps_of(rng, shape, pieces, least, top_value):
    loudness, own = 1.0, jax.random.fold_in(rng, 6)
    for axis_at, blocks in pieces:
        draws = jnp.exp(jax.random.uniform(jax.random.fold_in(own, axis_at), (blocks,), jnp.float32, least / len(pieces), top_value / len(pieces)))
        loudness = loudness * jnp.repeat(draws, shape[axis_at] // blocks).reshape([-1 if axis == axis_at else 1 for axis in range(len(shape))])
    return loudness


def scatter_about(own_key, shape, spread, bound, cuts=(), kind=jnp.bfloat16):
    entries = spread * jax.random.normal(own_key, shape, jnp.float32)
    if cuts:
        entries = entries * steps_of(own_key, shape, cuts, -0.22, 0.18)
    return jnp.clip(entries, -bound, bound).astype(kind)


def setup_inputs(seed: int = 0) -> dict:
    keys = jax.random.split(jax.random.key(seed), 18)
    return {
        "tokens": scatter_about(keys[0], (TOKENS, D), 0.5, 3.0, ((0, 16),)),
        "mixer_gain": jnp.clip(1.0 + 0.18 * jax.random.normal(keys[1], (D,), jnp.float32), 0.1, 1.9),
        "mix_weight": scatter_about(keys[2], (D, LRU), D ** -0.5, 0.125, ((0, 8), (1, 2))),
        "mixer_conv": scatter_about(keys[3], (MIX_TAPS, LRU), MIX_TAPS ** -0.5, 3.0, ((1, 2),), jnp.float32),
        "mixer_offset": scatter_about(keys[4], (LRU,), 0.02, 0.06, ((0, 2),), jnp.float32),
        "recur_weight": scatter_about(keys[5], (BLOCKS, BLOCK_DIM, BLOCK_DIM), BLOCK_DIM ** -0.5, 0.5, ((0, 2),)),
        "recur_bias": scatter_about(keys[6], (LRU,), 0.5, 3.0, ((0, 2),), jnp.float32),
        "input_weight": scatter_about(keys[7], (BLOCKS, BLOCK_DIM, BLOCK_DIM), BLOCK_DIM ** -0.5, 0.5, ((0, 2),)),
        "input_bias": jnp.clip(1.0 + 2.0 * jax.random.uniform(keys[8], (LRU,), jnp.float32) ** steps_of(keys[8], (LRU,), ((0, 2),), -0.2, 0.2), 1.0, 3.0),
        "decay_logit": draw_decay_logit(jax.random.fold_in(keys[17], 71), 0),
        "out_weight": scatter_about(keys[10], (LRU, D), (LRU // 4) ** -0.5, 0.375, ((0, 2), (1, 8))),
        "channel_gain": jnp.clip(1.0 + 0.18 * jax.random.normal(keys[11], (D,), jnp.float32), 0.1, 1.9),
        "gate_weight": scatter_about(keys[12], (D, FF), D ** -0.5, 0.125, ((0, 8), (1, 2))),
        "up_weight": scatter_about(keys[13], (D, FF), D ** -0.5, 0.125, ((0, 8), (1, 2))),
        "gate_conv": scatter_about(keys[14], (MLP_TAPS, FF), MLP_TAPS ** -0.5, 3.5, ((1, 2),), jnp.float32),
        "gate_offset": scatter_about(keys[15], (FF,), 0.5, 3.0, ((0, 2),), jnp.float32),
        "down_weight": scatter_about(keys[16], (FF, D), FF ** -0.5, 0.078125, ((0, 2), (1, 8))),
    }


epsilon = 1e-06
lru_scale = 8.0

def rms_rows(values, gain_row):
    widened = values.astype(jnp.float32)
    scaled = widened * lax.rsqrt(lax.optimization_barrier(jnp.mean(widened * widened, axis=-1, keepdims=True)) + epsilon)
    return (scaled * gain_row).astype(jnp.bfloat16)

def causal_conv(values, tap_rows, offset):
    width = tap_rows.shape[0]
    length = values.shape[-2]
    padding = [(0, 0)] * (values.ndim - 2) + [(width - 1, 0), (0, 0)]
    padded = jnp.pad(values, padding)
    total = offset + padded[..., 0:length, :] * tap_rows[0]
    for tap_index in range(1, width):
        total = total + padded[..., tap_index:tap_index + length, :] * tap_rows[tap_index]
    return total

def linear_combine(earlier, latter):
    decay_early, sum_early = earlier
    decay_late, sum_late = latter
    return (decay_early * decay_late, decay_late * sum_early + sum_late)

def lru_recur(recur_gate, input_gate, smoothed, decay_logit, axis):
    log_decay = lru_scale * recur_gate * jax.nn.log_sigmoid(decay_logit)
    drive = jnp.sqrt(-jnp.expm1(2.0 * log_decay)) * (input_gate * smoothed.astype(jnp.float32))
    _, states = lax.associative_scan(linear_combine, (jnp.exp(log_decay), drive), axis=axis)
    return states.astype(jnp.bfloat16)

def group_sums(left, right, groups):
    width = left.shape[1] // groups

    def add_group(total, index):
        left_part = lax.dynamic_slice_in_dim(left, index * width, width, 1)
        right_part = lax.dynamic_slice_in_dim(right, index * width, width, 0)
        partial_sum = jnp.dot(left_part, right_part, preferred_element_type=jnp.float32)
        rounded = lax.optimization_barrier(partial_sum.astype(jnp.bfloat16))
        return (total + rounded.astype(jnp.float32), None)
    start_total = jnp.zeros((left.shape[0], right.shape[1]), jnp.float32)
    total, _ = lax.scan(add_group, start_total, jnp.arange(groups, dtype=jnp.int32))
    return total

def block_gate(blocked, weight, bias):
    product = jnp.einsum('slhi,hij->slhj', blocked, weight.astype(jnp.float32))
    return jax.nn.sigmoid(product.reshape(SEQS, SEQLEN, LRU) + bias)

def reference(tokens, mixer_gain, mix_weight, mixer_conv, mixer_offset, recur_weight, recur_bias, input_weight, input_bias, decay_logit, out_weight, channel_gain, gate_weight, up_weight, gate_conv, gate_offset, down_weight):
    normed = rms_rows(tokens, mixer_gain)
    branch = jnp.dot(normed, mix_weight, preferred_element_type=jnp.float32).astype(jnp.bfloat16)
    branch = branch.reshape(SEQS, SEQLEN, LRU)
    smoothed = causal_conv(branch.astype(jnp.float32), mixer_conv, mixer_offset).astype(jnp.bfloat16)
    blocked = smoothed.reshape(SEQS, SEQLEN, BLOCKS, BLOCK_DIM).astype(jnp.float32)
    recur_gate = block_gate(blocked, recur_weight, recur_bias)
    input_gate = block_gate(blocked, input_weight, input_bias)
    recurrent = lru_recur(recur_gate, input_gate, smoothed, decay_logit, 1).reshape(TOKENS, LRU)
    mixer_sum = group_sums(recurrent, out_weight, N_TP)
    residual = (tokens.astype(jnp.float32) + mixer_sum).astype(jnp.bfloat16)
    normed_mlp = rms_rows(residual, channel_gain)
    gate_rows = jnp.dot(normed_mlp, gate_weight, preferred_element_type=jnp.float32).astype(jnp.bfloat16)
    up_rows = jnp.dot(normed_mlp, up_weight, preferred_element_type=jnp.float32).astype(jnp.bfloat16)
    gate_mixed = causal_conv(gate_rows.reshape(SEQS, SEQLEN, FF).astype(jnp.float32), gate_conv, gate_offset)
    hidden = jax.nn.gelu(gate_mixed) * up_rows.reshape(SEQS, SEQLEN, FF).astype(jnp.float32)
    hidden = hidden.astype(jnp.bfloat16).reshape(TOKENS, FF)
    mlp_sum = group_sums(hidden, down_weight, N_TP)
    return (residual.astype(jnp.float32) + mlp_sum).astype(jnp.bfloat16)
```

```python
import functools

import jax
import jax.numpy as jnp
from jax import lax
from jax.experimental import pallas as pl
from jax.experimental.pallas import tpu as pltpu
from jax.sharding import PartitionSpec as P

epsilon = 1e-06
lru_scale = 8.0


def rms_rows(values, gain_row):
    widened = values.astype(jnp.float32)
    scaled = widened * lax.rsqrt(jnp.mean(widened * widened, axis=-1, keepdims=True) + epsilon)
    return (scaled * gain_row).astype(jnp.bfloat16)


def causal_conv(values, tap_rows, offset):
    width = tap_rows.shape[0]
    length = values.shape[-2]
    padding = [(0, 0)] * (values.ndim - 2) + [(width - 1, 0), (0, 0)]
    padded = jnp.pad(values, padding)
    total = offset + padded[..., 0:length, :] * tap_rows[0]
    for tap_index in range(1, width):
        total = total + padded[..., tap_index : tap_index + length, :] * tap_rows[tap_index]
    return total


def one_minus_exp(v):
    series = 1.0 + v * (1.0 / 7.0)
    for order in (6.0, 5.0, 4.0, 3.0, 2.0):
        series = 1.0 + v * (1.0 / order) * series
    return jnp.where(v > -0.25, -v * series, 1.0 - jnp.exp(v))


def mixer_kernel(
    branch_ref, taps_ref, offset_ref, recur_ref, recur_bias_ref, input_ref, input_bias_ref, rate_ref, out_ref
):
    branch = branch_ref[...].astype(jnp.float32)
    length = branch.shape[0]
    width = taps_ref.shape[0]
    rows = lax.broadcasted_iota(jnp.int32, branch.shape, 0)

    def shifted(values, step, fill):
        return jnp.where(rows >= step, pltpu.roll(values, step, 0), fill)

    total = offset_ref[...] + branch * taps_ref[width - 1 : width, :]
    for back in range(1, width):
        total = total + shifted(branch, back, 0.0) * taps_ref[width - 1 - back : width - back, :]
    smoothed = total.astype(jnp.bfloat16)
    recur = jnp.dot(smoothed, recur_ref[0], preferred_element_type=jnp.float32)
    recur_gate = jax.nn.sigmoid(recur + recur_bias_ref[...])
    gated = jnp.dot(smoothed, input_ref[0], preferred_element_type=jnp.float32)
    input_gate = jax.nn.sigmoid(gated + input_bias_ref[...])
    log_decay = recur_gate * rate_ref[...]
    state = jnp.sqrt(one_minus_exp(2.0 * log_decay)) * (input_gate * smoothed.astype(jnp.float32))
    decay = jnp.exp(log_decay)
    step = 1
    while step < length:
        state = state + decay * shifted(state, step, 0.0)
        if 2 * step < length:
            decay = decay * shifted(decay, step, 1.0)
        step *= 2
    out_ref[...] = state.astype(jnp.bfloat16)


def mixer(branch, taps, offset, recur_weight, recur_bias, input_weight, input_bias, rate):
    length, channels = branch.shape
    blocks, dim, _ = recur_weight.shape
    column = lambda rows: pl.BlockSpec((rows, dim), lambda k: (0, k))
    square = pl.BlockSpec((1, dim, dim), lambda k: (k, 0, 0))
    row = lambda v: v.reshape(1, channels)
    return pl.pallas_call(
        mixer_kernel,
        name="mixer",
        grid=(blocks,),
        in_specs=[
            column(length),
            column(taps.shape[0]),
            column(1),
            square,
            column(1),
            square,
            column(1),
            column(1),
        ],
        out_specs=column(length),
        out_shape=jax.ShapeDtypeStruct((length, channels), jnp.bfloat16),
        cost_estimate=pl.CostEstimate(
            flops=60 * length * channels + 4 * length * channels * dim,
            bytes_accessed=4 * length * channels,
            transcendentals=5 * length * channels,
        ),
    )(
        branch,
        taps,
        row(offset),
        recur_weight,
        row(recur_bias),
        input_weight,
        row(input_bias),
        row(rate),
    )


def shift(values, axis, count, step):
    return lax.ppermute(values, axis, [(i, (i + step) % count) for i in range(count)])


def take(values, index, size, axis=0):
    return lax.dynamic_slice_in_dim(values, index * size, size, axis)


def pair_gather(weight, count, axis):
    groups = [list(range(parity, count, 2)) for parity in range(2)]
    own = lax.all_gather(weight, "fs", axis=axis, axis_index_groups=groups, tiled=True)
    other = lax.ppermute(own, "fs", [(i, i ^ 1) for i in range(count)])
    return own, other


def pair_columns(values, count, parity):
    rows, width = values.shape
    size = width // count
    blocks = [values[:, i * size : (i + 1) * size] for i in range(count)]
    even = jnp.concatenate(blocks[0::2], axis=1)
    odd = jnp.concatenate(blocks[1::2], axis=1)
    return jnp.where(parity == 0, even, odd), jnp.where(parity == 0, odd, even)


def scatter_rows(partial, n_tp, me):
    size = partial.shape[0] // n_tp
    total = take(partial, me, size).astype(jnp.float32)
    for step in range(1, n_tp):
        sent = take(partial, lax.rem(me + step, n_tp), size)
        total = total + shift(sent, "tp", n_tp, step).astype(jnp.float32)
    return total


def collect_rows(share, n_tp, me):
    size = share.shape[0]
    if n_tp == 2:
        other = shift(share, "tp", n_tp, 1)
        first = jnp.where(me == 0, share, other)
        second = jnp.where(me == 0, other, share)
        return jnp.concatenate([first, second], axis=0)
    whole = jnp.zeros((size * n_tp, share.shape[1]), share.dtype)
    whole = lax.dynamic_update_slice_in_dim(whole, share, me * size, 0)
    for step in range(1, n_tp):
        got = shift(share, "tp", n_tp, step)
        whole = lax.dynamic_update_slice_in_dim(whole, got, lax.rem(me - step + n_tp, n_tp) * size, 0)
    return whole


def plain(
    n_rep,
    n_fs,
    n_tp,
    tokens,
    mixer_gain,
    mix_weight,
    mixer_conv,
    mixer_offset,
    recur_weight,
    recur_bias,
    input_weight,
    input_bias,
    decay_logit,
    out_weight,
    channel_gain,
    gate_weight,
    up_weight,
    gate_conv,
    gate_offset,
    down_weight,
):
    rep = lax.axis_index("rep")
    tp = lax.axis_index("tp")
    parity = lax.rem(lax.axis_index("fs"), 2)
    length = tokens.shape[0]
    units = gate_weight.shape[1] // n_rep

    both = jnp.concatenate([mix_weight, out_weight.T], axis=1)
    both_full = lax.all_gather(both, "fs", axis=0, tiled=True)
    channels = mix_weight.shape[1]
    mixer_full, out_full = both_full[:, :channels], both_full[:, channels:]
    gate_own, gate_other = pair_gather(take(gate_weight, rep, units, 1), n_fs, 0)
    up_own, up_other = pair_gather(take(up_weight, rep, units, 1), n_fs, 0)
    down_full = lax.all_gather(take(down_weight, rep, units, 0), "fs", axis=1, tiled=True)
    gate_taps = take(gate_conv, rep, units, 1)
    gate_base = take(gate_offset, rep, units, 0)

    normed = rms_rows(tokens, mixer_gain)
    branch = jnp.dot(normed, mixer_full, preferred_element_type=jnp.float32).astype(jnp.bfloat16)
    recurrent = mixer(
        branch,
        mixer_conv,
        mixer_offset,
        recur_weight,
        recur_bias,
        input_weight,
        input_bias,
        lru_scale * jax.nn.log_sigmoid(decay_logit),
    )
    mixer_term = lax.dot_general(
        recurrent, out_full, (((1,), (1,)), ((), ())), preferred_element_type=jnp.float32
    )
    mixer_share = scatter_rows(mixer_term.astype(jnp.bfloat16), n_tp, tp)
    rows = length // n_tp
    residual = (take(tokens, tp, rows).astype(jnp.float32) + mixer_share).astype(jnp.bfloat16)
    normed_share = rms_rows(residual, channel_gain)

    shares = [normed_share]
    for step in range(1, n_rep):
        shares.append(shift(normed_share, "rep", n_rep, step))

    def channel_mixer(share):
        rows_in = collect_rows(share, n_tp, tp)
        left, right = pair_columns(rows_in, n_fs, parity)
        gate_rows = jnp.dot(left, gate_own, preferred_element_type=jnp.float32)
        gate_rows = gate_rows + jnp.dot(right, gate_other, preferred_element_type=jnp.float32)
        up_rows = jnp.dot(left, up_own, preferred_element_type=jnp.float32)
        up_rows = up_rows + jnp.dot(right, up_other, preferred_element_type=jnp.float32)
        gate_rows = gate_rows.astype(jnp.bfloat16)
        up_rows = up_rows.astype(jnp.bfloat16)
        gate_mixed = causal_conv(gate_rows.astype(jnp.float32), gate_taps, gate_base)
        hidden = (jax.nn.gelu(gate_mixed) * up_rows.astype(jnp.float32)).astype(jnp.bfloat16)
        return jnp.dot(hidden, down_full, preferred_element_type=jnp.float32).astype(jnp.bfloat16)

    own_terms = channel_mixer(shares[0])
    total = None
    for step in range(1, n_rep):
        summed = scatter_rows(channel_mixer(shares[step]), n_tp, tp).astype(jnp.bfloat16)
        back = shift(summed, "rep", n_rep, -step).astype(jnp.float32)
        total = back if total is None else total + back
    own = scatter_rows(own_terms, n_tp, tp)
    total = own if total is None else own + total
    result = (residual.astype(jnp.float32) + total).astype(jnp.bfloat16)
    return collect_rows(result, n_tp, tp)


MESH = pl.DeviceIdType.MESH
unit_tile = 256


class Copies:
    def __init__(self, send_sem):
        self.send_sem = send_sem
        self.made = []

    def send(self, src, dst, recv_sem, device, cond=None, now=None):
        index = len(self.made)
        assert index < self.send_sem.shape[0]

        def make():
            return pltpu.make_async_remote_copy(
                src_ref=src(),
                dst_ref=dst(),
                send_sem=self.send_sem.at[index],
                recv_sem=recv_sem(),
                device_id=device,
                device_id_type=MESH,
            )

        self.made.append((make, cond))
        guarded(both_of(cond, now), lambda: make().start())

    def drain(self):
        for make, cond in self.made:
            guarded(cond, lambda make=make: make().wait_send())


def guarded(cond, act):
    if cond is None:
        act()
    else:
        pl.when(cond)(lambda: act())


def both_of(first, second):
    if first is None or second is None:
        return second if first is None else first
    return jnp.logical_and(first, second)


def rows_at(start, size):
    if isinstance(start, int):
        return pl.ds(start, size)
    return pl.ds(pl.multiple_of(start, size), size)


def send_count(n_z, chunks):
    mixer = 4 + 10 * (n_z - 1)
    weights = (chunks + 1) * (1 + 2 * (n_z - 1) + 2)
    return mixer + weights + 1 + 4 + 3


def layer_kernel(
    n_z,
    tokens,
    mixer_gain,
    mix_w,
    taps,
    offset,
    recur_w,
    recur_b,
    input_w,
    input_b,
    rate,
    out_w,
    channel_gain,
    gate_w,
    up_w,
    gate_taps,
    gate_base,
    down_w,
    out,
    tok,
    mixb,
    outb,
    branch,
    recurrent,
    term_send,
    term_recv,
    term_own,
    residual,
    acts,
    gub,
    gub_swap,
    dnb,
    dnb_swap,
    hid,
    half_send,
    half_recv,
    half_own,
    chip_own,
    chip_send,
    chip_recv,
    result,
    local_sem,
    send_sem,
    mix_sem,
    gu_sem,
    dn_sem,
    term_sem,
    act_sem,
    half_send_sem,
    half_recv_sem,
    chip_send_sem,
    chip_recv_sem,
    out_send_sem,
    out_recv_sem,
):
    x = lax.axis_index("rep")
    f = lax.axis_index("fs")
    t = lax.axis_index("tp")
    z, y = f // 2, f % 2
    n_f = 2 * n_z
    length, width = tokens.shape
    depth, channels = mix_w.shape
    chunks = gub.shape[0]
    units = chunks * unit_tile
    half = length // 2
    dim = recur_w.shape[1]

    def at(x_at, z_at, y_at, t_at):
        return (x_at, z_at * 2 + y_at, t_at)

    other_x, other_y, other_t = 1 - x, 1 - y, 1 - t
    near = {1: at(other_x, z, y, t), 2: at(x, z, other_y, t), 3: at(other_x, z, other_y, t)}
    partner = at(x, z, y, other_t)
    beside = z * 2 + other_y
    column = [(z + step) % n_z for step in range(n_z)]
    edge = n_z - 1
    relay = n_z == 4
    is_mid = jnp.logical_and(z > 0, z < edge) if relay else None
    mid_from = edge - z
    mid_blocks = [mid_from * 2 + y, mid_from * 2 + other_y]
    mid_device = at(x, jnp.where(z == 1, 0, edge), y, t)

    def direct(step):
        if relay and step == 2:
            return jnp.logical_not(is_mid)
        return None

    quarter = x * 2 + y
    quarter_swap = x * 2 + other_y
    local = []

    def bring(src, dst):
        copy = pltpu.make_async_copy(src, dst, local_sem.at[len(local)])
        copy.start()
        local.append(copy)
        return copy

    own_rows = rows_at(f * depth, depth)
    got_mix = [bring(mix_w, mixb.at[own_rows, :]), bring(out_w, outb.at[:, own_rows])]

    def unit_cols(which, chunk):
        return rows_at(which * units + chunk * unit_tile, unit_tile)

    low, high = pl.ds(0, unit_tile), pl.ds(unit_tile, unit_tile)
    got_own, got_swap = [], []
    for c in range(chunks):
        got_own.append(
            [
                bring(gate_w.at[:, unit_cols(quarter, c)], gub.at[c, own_rows, low]),
                bring(up_w.at[:, unit_cols(quarter, c)], gub.at[c, own_rows, high]),
            ]
        )
        got_swap.append(
            [
                bring(gate_w.at[:, unit_cols(quarter_swap, c)], gub_swap.at[c, :, low]),
                bring(up_w.at[:, unit_cols(quarter_swap, c)], gub_swap.at[c, :, high]),
            ]
        )
    got_tok = [bring(tokens, tok)]
    got_own.append([bring(down_w.at[rows_at(quarter * units, units), :], dnb.at[f])])
    got_swap.append([bring(down_w.at[rows_at(quarter_swap * units, units), :], dnb_swap)])

    barrier = pltpu.get_barrier_semaphore()
    peers = [near[1], near[2], near[3], partner] + [at(x, w, y, t) for w in column[1:]]
    for peer in peers:
        pl.semaphore_signal(barrier, inc=1, device_id=peer, device_id_type=MESH)
    pl.semaphore_wait(barrier, len(peers))

    copies = Copies(send_sem)

    def arrived(dst, sem, cond=None):
        def wait():
            copy = pltpu.make_async_remote_copy(
                src_ref=dst(),
                dst_ref=dst(),
                send_sem=sem(),
                recv_sem=sem(),
                device_id=partner,
                device_id_type=MESH,
            )
            copy.wait_recv()

        guarded(cond, wait)

    part_rows, part_out = depth // 2, channels // 2

    def mix_pieces(block, part):
        return [
            (
                lambda: mixb.at[rows_at(block * depth + part * part_rows, part_rows), :],
                lambda: mix_sem.at[block, 2 * part],
            ),
            (
                lambda: outb.at[rows_at(part * part_out, part_out), rows_at(block * depth, depth)],
                lambda: mix_sem.at[block, 2 * part + 1],
            ),
        ]

    def send_mix(block, part, device, cond=None):
        for ref, sem in mix_pieces(block, part):
            copies.send(ref, ref, sem, device, cond)

    def wait_mix(block, part):
        for ref, sem in mix_pieces(block, part):
            arrived(ref, sem)

    def weight_ref(stage, block):
        if stage == chunks:
            return lambda: dnb.at[block], lambda: dn_sem.at[block]
        return lambda: gub.at[stage, rows_at(block * depth, depth), :], lambda: gu_sem.at[stage, block]

    def send_swap(stage):
        for copy in got_swap[stage]:
            copy.wait()
        ref, sem = weight_ref(stage, f)
        copies.send(lambda: dnb_swap if stage == chunks else gub_swap.at[stage], ref, sem, near[2])

    def send_own(stage):
        for copy in got_own[stage]:
            copy.wait()
        ref, sem = weight_ref(stage, f)
        for step in range(1, n_z):
            copies.send(ref, ref, sem, at(x, column[step], y, t), direct(step))

    def send_beside(stage):
        ref, sem = weight_ref(stage, beside)
        arrived(ref, sem)
        for step in range(1, n_z):
            copies.send(ref, ref, sem, at(x, column[step], y, t), direct(step))

    def relay_block(stage, side, now=None):
        if relay:
            ref, sem = weight_ref(stage, mid_blocks[side])
            arrived(ref, sem, both_of(is_mid, now))
            copies.send(ref, ref, sem, mid_device, is_mid, now)

    def wait_stage(stage, now=None):
        for step in range(1, n_z):
            for side in (y, other_y):
                ref, sem = weight_ref(stage, column[step] * 2 + side)
                fresh = None
                if relay:
                    fresh = jnp.logical_not(jnp.logical_and(is_mid, column[step] == mid_from))
                arrived(ref, sem, both_of(fresh, now))

    for copy in got_mix:
        copy.wait()
    for step in range(1, n_z):
        send_mix(f, x, at(x, column[step], y, t), direct(step))
    for part in range(2):
        send_mix(f, part, near[2])
    send_own(0)
    send_swap(0)

    def norm_rows(source, gain, dest, total, size=64):
        def body(i, carry):
            at_rows = rows_at(i * size, size)
            widened = source[at_rows, :].astype(jnp.float32)
            scaled = widened * lax.rsqrt(jnp.mean(widened * widened, axis=-1, keepdims=True) + epsilon)
            dest[at_rows, :] = (scaled * gain[...]).astype(jnp.bfloat16)
            return carry

        lax.fori_loop(0, total // size, body, 0)

    for copy in got_tok:
        copy.wait()
    norm_rows(tok, mixer_gain, acts.at[0], length)

    order = [step for pair in zip(range(1, n_z), range(n_z - 1, 0, -1)) for step in pair][: n_z - 1]
    for step in order:
        block = column[step] * 2 + y
        wait_mix(block, x)
        send_mix(block, x, near[2])
        send_mix(block, x, near[1])
        if relay:
            send_mix(block, x, mid_device, jnp.logical_and(is_mid, column[step] == mid_from))
    for stage in range(1, chunks + 1):
        send_swap(stage)
    send_beside(0)
    send_own(1)
    for step in order:
        block = column[step] * 2 + other_y
        wait_mix(block, x)
        send_mix(block, x, near[1])
    send_beside(1)
    relay_block(0, 0)
    for stage in range(2, chunks):
        send_own(stage)
        send_beside(stage)
    send_own(chunks)
    relay_block(0, 1)
    for part in range(2):
        wait_mix(beside, part)
    for step in order:
        for side in (y, other_y):
            wait_mix(column[step] * 2 + side, other_x)

    def branch_body(j, carry):
        cols = rows_at(j * 256, 256)
        branch[:, cols] = (
            jnp.dot(acts[0], mixb[:, cols], preferred_element_type=jnp.float32).astype(jnp.bfloat16).astype(jnp.float32)
        )
        return carry

    lax.fori_loop(0, channels // 256, branch_body, 0)

    def block_body(k, carry):
        cols = rows_at(k * dim, dim)
        recurrent[:, cols] = recur_block(
            branch[:, cols],
            taps[:, cols],
            offset[:, cols],
            recur_w[k],
            recur_b[:, cols],
            input_w[k],
            input_b[:, cols],
            rate[:, cols],
        )
        return carry

    lax.fori_loop(0, channels // dim, block_body, 0)

    def project(which, dest):
        rows = rows_at(which * half, half)

        def body(j, carry):
            cols = rows_at(j * 512, 512)
            dest[:, cols] = jnp.dot(recurrent[rows, :], outb[:, cols], preferred_element_type=jnp.float32).astype(
                jnp.bfloat16
            )
            return carry

        lax.fori_loop(0, width // 512, body, 0)

    project(other_t, term_send)
    copies.send(lambda: term_send, lambda: term_recv, lambda: term_sem.at[0], partner)
    send_beside(chunks)
    if chunks > 1:
        relay_block(1, 0)
    project(t, term_own)
    arrived(lambda: term_recv, lambda: term_sem.at[0])
    mine = rows_at(t * half, half)
    theirs = rows_at(other_t * half, half)

    def residual_body(i, carry):
        rows = rows_at(i * 64, 64)
        total = term_own[rows, :].astype(jnp.float32) + term_recv[rows, :].astype(jnp.float32)
        base = tok[rows_at(t * half + i * 64, 64), :].astype(jnp.float32)
        residual[rows, :] = (base + total).astype(jnp.bfloat16)
        return carry

    lax.fori_loop(0, half // 64, residual_body, 0)
    norm_rows(residual, channel_gain, acts.at[0, mine, :], half)
    def act_part(slot, rows):
        return lambda: acts.at[slot, rows, :]

    def act_arrival(slot, hop):
        return lambda: act_sem.at[slot, hop]

    for slot in (1, 2, 3):
        copies.send(act_part(0, mine), act_part(slot, mine), act_arrival(slot, 0), near[slot])
    copies.send(act_part(0, mine), act_part(0, mine), act_arrival(0, 1), partner)
    if chunks > 1:
        relay_block(1, 1)

    def pass_on(slot, now):
        arrived(act_part(slot, mine), act_arrival(slot, 0), now)
        copies.send(act_part(slot, mine), act_part(slot, mine), act_arrival(slot, 1), partner, None, now)

    def wait_acts(slot, now):
        arrived(act_part(slot, theirs), act_arrival(slot, 1), now)

    early = max(chunks - 1, 1)
    plan = [(slot, c) for slot in range(4) for c in range(early)]
    plan += [(slot, c) for c in range(early, chunks) for slot in range(4)]
    hooks = [[] for _ in plan]
    for number, (slot, c) in enumerate(plan):
        if slot == 0:
            hooks[number].append(functools.partial(wait_stage, c))
        if c == 0:
            hooks[number].append(functools.partial(wait_acts, slot))
    for slot in (1, 2, 3):
        hooks[slot * early - 1].append(functools.partial(pass_on, slot))
    for stage in range(2, chunks + 1):
        for side in range(2):
            hooks[min(2 * stage - 2, len(plan) - 1)].append(functools.partial(relay_block, stage, side))

    rows_iota = lax.broadcasted_iota(jnp.int32, (length, unit_tile), 0)

    def gate_body(number, carry):
        late = number >= 4 * early
        slot = jnp.where(late, (number - 4 * early) % 4, number // early)
        c = jnp.where(late, early + (number - 4 * early) // 4, number % early)
        for index, acting in enumerate(hooks):
            for act in acting:
                act(now=number == index)

        both = jnp.dot(acts[slot], gub[c], preferred_element_type=jnp.float32)
        gate = both[:, :unit_tile].astype(jnp.bfloat16).astype(jnp.float32)
        up = both[:, unit_tile:].astype(jnp.bfloat16).astype(jnp.float32)
        cols = rows_at(quarter * units + c * unit_tile, unit_tile)
        width_taps = gate_taps.shape[0]
        mixed = gate_base[:, cols] + gate * gate_taps[width_taps - 1 : width_taps, cols]
        for back in range(1, width_taps):
            moved = jnp.where(rows_iota >= back, pltpu.roll(gate, back, 0), 0.0)
            mixed = mixed + moved * gate_taps[width_taps - 1 - back : width_taps - back, cols]
        hidden = (jax.nn.gelu(mixed) * up).astype(jnp.bfloat16)
        place = rows_at(c * unit_tile, unit_tile)
        rows = rows_at(slot * half, half)
        hid[0, rows, place] = hidden[:half]
        hid[1, rows, place] = hidden[half:]
        return carry

    lax.fori_loop(0, len(plan), gate_body, 0)

    def block_of(i):
        k = i // 2
        if n_z == 4:
            return (((z // 2 + k // 2) % 2) * 2 + (z % 2 + k % 2) % 2) * 2 + i % 2
        return ((z + k) % n_z) * 2 + i % 2

    def half_copy(i):
        return pltpu.make_async_remote_copy(
            src_ref=half_send.at[i],
            dst_ref=half_recv.at[i],
            send_sem=half_send_sem.at[i],
            recv_sem=half_recv_sem.at[i],
            device_id=partner,
            device_id_type=MESH,
        )

    def chip_copy(i, slot):
        return pltpu.make_async_remote_copy(
            src_ref=chip_send.at[i, slot - 1],
            dst_ref=chip_recv.at[i, slot - 1],
            send_sem=chip_send_sem.at[i, slot - 1],
            recv_sem=chip_recv_sem.at[i, slot - 1],
            device_id=near[slot],
            device_id_type=MESH,
        )

    def out_copy(i):
        part = result.at[mine, rows_at(block_of(i) * depth, depth)]
        return pltpu.make_async_remote_copy(
            src_ref=part,
            dst_ref=part,
            send_sem=out_send_sem.at[i],
            recv_sem=out_recv_sem.at[i],
            device_id=partner,
            device_id_type=MESH,
        )

    lag = 3

    def down_body(i, carry):
        @pl.when(i < n_f)
        def _():
            block = block_of(i)
            known = jnp.logical_or(block == f, block == beside)
            if relay:
                known = jnp.logical_or(known, jnp.logical_and(is_mid, block // 2 == mid_from))
            arrived(lambda: dnb.at[block], lambda: dn_sem.at[block], jnp.logical_not(known))
            half_send[i] = jnp.dot(hid[other_t], dnb[block], preferred_element_type=jnp.float32).astype(jnp.bfloat16)
            half_copy(i).start()
            half_own[i % 2] = jnp.dot(hid[t], dnb[block], preferred_element_type=jnp.float32).astype(jnp.bfloat16)

        j = i - 1

        @pl.when(jnp.logical_and(j >= 0, j < n_f))
        def _():
            half_copy(j).wait_recv()

            def add(slot):
                rows = pl.ds(slot * half, half)
                return half_own[j % 2, rows, :].astype(jnp.float32) + half_recv[j, rows, :].astype(jnp.float32)

            for slot in (3, 1, 2):
                chip_send[j, slot - 1] = add(slot).astype(jnp.bfloat16)
            for slot in (1, 2, 3):
                chip_copy(j, slot).start()
            chip_own[j] = add(0)

        m = i - lag

        @pl.when(m >= 0)
        def _():
            for slot in (1, 2, 3):
                chip_copy(m, slot).wait_recv()
            cols = rows_at(block_of(m) * depth, depth)
            total = chip_own[m]
            for slot in range(3):
                total = total + chip_recv[m, slot].astype(jnp.float32)
            result[mine, cols] = (residual[:, cols].astype(jnp.float32) + total).astype(jnp.bfloat16)
            out_copy(m).start()

        return carry

    lax.fori_loop(0, n_f + lag, down_body, 0)

    def drain_body(i, carry):
        out_copy(i).wait_send()
        half_copy(i).wait_send()
        for slot in (1, 2, 3):
            chip_copy(i, slot).wait_send()
        arrived(
            lambda: result.at[theirs, rows_at(block_of(i) * depth, depth)],
            lambda: out_recv_sem.at[i],
        )
        return carry

    lax.fori_loop(0, n_f, drain_body, 0)
    copies.drain()
    last = pltpu.make_async_copy(result, out, local_sem.at[len(local)])
    last.start()
    last.wait()


def recur_block(branch, taps, offset, recur_weight, recur_bias, input_weight, input_bias, rate):
    length = branch.shape[0]
    width = taps.shape[0]
    rows = lax.broadcasted_iota(jnp.int32, branch.shape, 0)

    def shifted(values, step, fill):
        return jnp.where(rows >= step, pltpu.roll(values, step, 0), fill)

    total = offset + branch * taps[width - 1 : width, :]
    for back in range(1, width):
        total = total + shifted(branch, back, 0.0) * taps[width - 1 - back : width - back, :]
    smoothed = total.astype(jnp.bfloat16)
    recur = jnp.dot(smoothed, recur_weight, preferred_element_type=jnp.float32)
    recur_gate = jax.nn.sigmoid(recur + recur_bias)
    gated = jnp.dot(smoothed, input_weight, preferred_element_type=jnp.float32)
    input_gate = jax.nn.sigmoid(gated + input_bias)
    log_decay = recur_gate * rate
    state = jnp.sqrt(one_minus_exp(2.0 * log_decay)) * (input_gate * smoothed.astype(jnp.float32))
    decay = jnp.exp(log_decay)
    step = 1
    while step < length:
        state = state + decay * shifted(state, step, 0.0)
        if 2 * step < length:
            decay = decay * shifted(decay, step, 1.0)
        step *= 2
    return state.astype(jnp.bfloat16)


def fused(
    n_fs,
    tokens,
    mixer_gain,
    mix_weight,
    mixer_conv,
    mixer_offset,
    recur_weight,
    recur_bias,
    input_weight,
    input_bias,
    decay_logit,
    out_weight,
    channel_gain,
    gate_weight,
    up_weight,
    gate_conv,
    gate_offset,
    down_weight,
):
    n_z = n_fs // 2
    length, width = tokens.shape
    depth, channels = mix_weight.shape
    units = gate_weight.shape[1] // 4
    chunks = units // unit_tile
    half = length // 2
    row = lambda v: v.reshape(1, v.shape[0])
    hbm = pl.BlockSpec(memory_space=pl.ANY)
    vmem = pl.BlockSpec(memory_space=pltpu.VMEM)
    bf16, f32 = jnp.bfloat16, jnp.float32
    dma = pltpu.SemaphoreType.DMA
    return pl.pallas_call(
        functools.partial(layer_kernel, n_z),
        name="layer",
        in_specs=[hbm, vmem, hbm] + [vmem] * 7 + [hbm, vmem, hbm, hbm, vmem, vmem, hbm],
        out_specs=hbm,
        out_shape=jax.ShapeDtypeStruct((length, width), bf16),
        scratch_shapes=[
            pltpu.VMEM((length, width), bf16),
            pltpu.VMEM((width, channels), bf16),
            pltpu.VMEM((channels, width), bf16),
            pltpu.VMEM((length, channels), f32),
            pltpu.VMEM((length, channels), bf16),
            pltpu.VMEM((half, width), bf16),
            pltpu.VMEM((half, width), bf16),
            pltpu.VMEM((half, width), bf16),
            pltpu.VMEM((half, width), bf16),
            pltpu.VMEM((4, length, width), bf16),
            pltpu.VMEM((chunks, width, 2 * unit_tile), bf16),
            pltpu.VMEM((chunks, depth, 2 * unit_tile), bf16),
            pltpu.VMEM((n_fs, units, depth), bf16),
            pltpu.VMEM((units, depth), bf16),
            pltpu.VMEM((2, 4 * half, units), bf16),
            pltpu.VMEM((n_fs, 4 * half, depth), bf16),
            pltpu.VMEM((n_fs, 4 * half, depth), bf16),
            pltpu.VMEM((2, 4 * half, depth), bf16),
            pltpu.VMEM((n_fs, half, depth), f32),
            pltpu.VMEM((n_fs, 3, half, depth), bf16),
            pltpu.VMEM((n_fs, 3, half, depth), bf16),
            pltpu.VMEM((length, width), bf16),
            dma((6 + 4 * chunks,)),
            dma((send_count(n_z, chunks),)),
            dma((n_fs, 4)),
            dma((chunks, n_fs)),
            dma((n_fs,)),
            dma((1,)),
            dma((4, 2)),
            dma((n_fs,)),
            dma((n_fs,)),
            dma((n_fs, 3)),
            dma((n_fs, 3)),
            dma((n_fs,)),
            dma((n_fs,)),
        ],
        compiler_params=pltpu.CompilerParams(
            collective_id=0, has_side_effects=True, vmem_limit_bytes=60 * 2**20
        ),
    )(
        tokens,
        row(mixer_gain),
        mix_weight,
        mixer_conv,
        row(mixer_offset),
        recur_weight,
        row(recur_bias),
        input_weight,
        row(input_bias),
        row(lru_scale * jax.nn.log_sigmoid(decay_logit)),
        out_weight,
        row(channel_gain),
        gate_weight,
        up_weight,
        gate_conv,
        row(gate_offset),
        down_weight,
    )


def local(n_rep, n_fs, n_tp, *arrays):
    units, columns = arrays[16].shape
    fits = n_rep == 2 and n_tp == 2 and n_fs % 2 == 0 and n_fs <= 8
    if fits and units % (4 * unit_tile) == 0 and columns % 128 == 0:
        return fused(n_fs, *arrays)
    return plain(n_rep, n_fs, n_tp, *arrays)


def solution(mesh):
    in_specs = (
        P(("rep", "fs"), None),
        P(),
        P("fs", "tp"),
        P(None, "tp"),
        P("tp"),
        P("tp", None, None),
        P("tp"),
        P("tp", None, None),
        P("tp"),
        P("tp"),
        P("tp", "fs"),
        P(),
        P("fs", "tp"),
        P("fs", "tp"),
        P(None, "tp"),
        P("tp"),
        P("tp", "fs"),
    )
    out_specs = P(("rep", "fs"), None)
    body = functools.partial(local, mesh.shape["rep"], mesh.shape["fs"], mesh.shape["tp"])
    return jax.shard_map(body, mesh=mesh, in_specs=in_specs, out_specs=out_specs, check_vma=False)
```

```python
import functools

import jax
import jax.numpy as jnp
from jax import lax
from jax.experimental import pallas as pl
from jax.experimental.pallas import tpu as pltpu
from jax.sharding import PartitionSpec as P

epsilon = 1e-06
lru_scale = 8.0


def rms_rows(values, gain_row):
    widened = values.astype(jnp.float32)
    scaled = widened * lax.rsqrt(jnp.mean(widened * widened, axis=-1, keepdims=True) + epsilon)
    return (scaled * gain_row).astype(jnp.bfloat16)


def causal_conv(values, tap_rows, offset):
    width = tap_rows.shape[0]
    length = values.shape[-2]
    padding = [(0, 0)] * (values.ndim - 2) + [(width - 1, 0), (0, 0)]
    padded = jnp.pad(values, padding)
    total = offset + padded[..., 0:length, :] * tap_rows[0]
    for tap_index in range(1, width):
        total = total + padded[..., tap_index : tap_index + length, :] * tap_rows[tap_index]
    return total


def one_minus_exp(v):
    series = 1.0 + v * (1.0 / 7.0)
    for order in (6.0, 5.0, 4.0, 3.0, 2.0):
        series = 1.0 + v * (1.0 / order) * series
    return jnp.where(v > -0.25, -v * series, 1.0 - jnp.exp(v))


def mixer_kernel(
    branch_ref, taps_ref, offset_ref, recur_ref, recur_bias_ref, input_ref, input_bias_ref, rate_ref, out_ref
):
    branch = branch_ref[...].astype(jnp.float32)
    length = branch.shape[0]
    width = taps_ref.shape[0]
    rows = lax.broadcasted_iota(jnp.int32, branch.shape, 0)

    def shifted(values, step, fill):
        return jnp.where(rows >= step, pltpu.roll(values, step, 0), fill)

    total = offset_ref[...] + branch * taps_ref[width - 1 : width, :]
    for back in range(1, width):
        total = total + shifted(branch, back, 0.0) * taps_ref[width - 1 - back : width - back, :]
    smoothed = total.astype(jnp.bfloat16)
    recur = jnp.dot(smoothed, recur_ref[0], preferred_element_type=jnp.float32)
    recur_gate = jax.nn.sigmoid(recur + recur_bias_ref[...])
    gated = jnp.dot(smoothed, input_ref[0], preferred_element_type=jnp.float32)
    input_gate = jax.nn.sigmoid(gated + input_bias_ref[...])
    log_decay = recur_gate * rate_ref[...]
    state = jnp.sqrt(one_minus_exp(2.0 * log_decay)) * (input_gate * smoothed.astype(jnp.float32))
    decay = jnp.exp(log_decay)
    step = 1
    while step < length:
        state = state + decay * shifted(state, step, 0.0)
        if 2 * step < length:
            decay = decay * shifted(decay, step, 1.0)
        step *= 2
    out_ref[...] = state.astype(jnp.bfloat16)


def mixer(branch, taps, offset, recur_weight, recur_bias, input_weight, input_bias, rate):
    length, channels = branch.shape
    blocks, dim, _ = recur_weight.shape
    column = lambda rows: pl.BlockSpec((rows, dim), lambda k: (0, k))
    square = pl.BlockSpec((1, dim, dim), lambda k: (k, 0, 0))
    row = lambda v: v.reshape(1, channels)
    return pl.pallas_call(
        mixer_kernel,
        name="mixer",
        grid=(blocks,),
        in_specs=[
            column(length),
            column(taps.shape[0]),
            column(1),
            square,
            column(1),
            square,
            column(1),
            column(1),
        ],
        out_specs=column(length),
        out_shape=jax.ShapeDtypeStruct((length, channels), jnp.bfloat16),
        cost_estimate=pl.CostEstimate(
            flops=60 * length * channels + 4 * length * channels * dim,
            bytes_accessed=4 * length * channels,
            transcendentals=5 * length * channels,
        ),
    )(
        branch,
        taps,
        row(offset),
        recur_weight,
        row(recur_bias),
        input_weight,
        row(input_bias),
        row(rate),
    )


def shift(values, axis, count, step):
    return lax.ppermute(values, axis, [(i, (i + step) % count) for i in range(count)])


def take(values, index, size, axis=0):
    return lax.dynamic_slice_in_dim(values, index * size, size, axis)


def pair_gather(weight, count, axis):
    groups = [list(range(parity, count, 2)) for parity in range(2)]
    own = lax.all_gather(weight, "fs", axis=axis, axis_index_groups=groups, tiled=True)
    other = lax.ppermute(own, "fs", [(i, i ^ 1) for i in range(count)])
    return own, other


def pair_columns(values, count, parity):
    rows, width = values.shape
    size = width // count
    blocks = [values[:, i * size : (i + 1) * size] for i in range(count)]
    even = jnp.concatenate(blocks[0::2], axis=1)
    odd = jnp.concatenate(blocks[1::2], axis=1)
    return jnp.where(parity == 0, even, odd), jnp.where(parity == 0, odd, even)


def scatter_rows(partial, n_tp, me):
    size = partial.shape[0] // n_tp
    total = take(partial, me, size).astype(jnp.float32)
    for step in range(1, n_tp):
        sent = take(partial, lax.rem(me + step, n_tp), size)
        total = total + shift(sent, "tp", n_tp, step).astype(jnp.float32)
    return total


def collect_rows(share, n_tp, me):
    size = share.shape[0]
    if n_tp == 2:
        other = shift(share, "tp", n_tp, 1)
        first = jnp.where(me == 0, share, other)
        second = jnp.where(me == 0, other, share)
        return jnp.concatenate([first, second], axis=0)
    whole = jnp.zeros((size * n_tp, share.shape[1]), share.dtype)
    whole = lax.dynamic_update_slice_in_dim(whole, share, me * size, 0)
    for step in range(1, n_tp):
        got = shift(share, "tp", n_tp, step)
        whole = lax.dynamic_update_slice_in_dim(whole, got, lax.rem(me - step + n_tp, n_tp) * size, 0)
    return whole


def plain(
    n_rep,
    n_fs,
    n_tp,
    tokens,
    mixer_gain,
    mix_weight,
    mixer_conv,
    mixer_offset,
    recur_weight,
    recur_bias,
    input_weight,
    input_bias,
    decay_logit,
    out_weight,
    channel_gain,
    gate_weight,
    up_weight,
    gate_conv,
    gate_offset,
    down_weight,
):
    rep = lax.axis_index("rep")
    tp = lax.axis_index("tp")
    parity = lax.rem(lax.axis_index("fs"), 2)
    length = tokens.shape[0]
    units = gate_weight.shape[1] // n_rep

    both = jnp.concatenate([mix_weight, out_weight.T], axis=1)
    both_full = lax.all_gather(both, "fs", axis=0, tiled=True)
    channels = mix_weight.shape[1]
    mixer_full, out_full = both_full[:, :channels], both_full[:, channels:]
    gate_own, gate_other = pair_gather(take(gate_weight, rep, units, 1), n_fs, 0)
    up_own, up_other = pair_gather(take(up_weight, rep, units, 1), n_fs, 0)
    down_full = lax.all_gather(take(down_weight, rep, units, 0), "fs", axis=1, tiled=True)
    gate_taps = take(gate_conv, rep, units, 1)
    gate_base = take(gate_offset, rep, units, 0)

    normed = rms_rows(tokens, mixer_gain)
    branch = jnp.dot(normed, mixer_full, preferred_element_type=jnp.float32).astype(jnp.bfloat16)
    recurrent = mixer(
        branch,
        mixer_conv,
        mixer_offset,
        recur_weight,
        recur_bias,
        input_weight,
        input_bias,
        lru_scale * jax.nn.log_sigmoid(decay_logit),
    )
    mixer_term = lax.dot_general(
        recurrent, out_full, (((1,), (1,)), ((), ())), preferred_element_type=jnp.float32
    )
    mixer_share = scatter_rows(mixer_term.astype(jnp.bfloat16), n_tp, tp)
    rows = length // n_tp
    residual = (take(tokens, tp, rows).astype(jnp.float32) + mixer_share).astype(jnp.bfloat16)
    normed_share = rms_rows(residual, channel_gain)

    shares = [normed_share]
    for step in range(1, n_rep):
        shares.append(shift(normed_share, "rep", n_rep, step))

    def channel_mixer(share):
        rows_in = collect_rows(share, n_tp, tp)
        left, right = pair_columns(rows_in, n_fs, parity)
        gate_rows = jnp.dot(left, gate_own, preferred_element_type=jnp.float32)
        gate_rows = gate_rows + jnp.dot(right, gate_other, preferred_element_type=jnp.float32)
        up_rows = jnp.dot(left, up_own, preferred_element_type=jnp.float32)
        up_rows = up_rows + jnp.dot(right, up_other, preferred_element_type=jnp.float32)
        gate_rows = gate_rows.astype(jnp.bfloat16)
        up_rows = up_rows.astype(jnp.bfloat16)
        gate_mixed = causal_conv(gate_rows.astype(jnp.float32), gate_taps, gate_base)
        hidden = (jax.nn.gelu(gate_mixed) * up_rows.astype(jnp.float32)).astype(jnp.bfloat16)
        return jnp.dot(hidden, down_full, preferred_element_type=jnp.float32).astype(jnp.bfloat16)

    own_terms = channel_mixer(shares[0])
    total = None
    for step in range(1, n_rep):
        summed = scatter_rows(channel_mixer(shares[step]), n_tp, tp).astype(jnp.bfloat16)
        back = shift(summed, "rep", n_rep, -step).astype(jnp.float32)
        total = back if total is None else total + back
    own = scatter_rows(own_terms, n_tp, tp)
    total = own if total is None else own + total
    result = (residual.astype(jnp.float32) + total).astype(jnp.bfloat16)
    return collect_rows(result, n_tp, tp)


MESH = pl.DeviceIdType.MESH
unit_tile = 256
pieces = 2


class Copies:
    def __init__(self, send_sem):
        self.send_sem = send_sem
        self.made = []

    def send(self, src, dst, recv_sem, device, cond=None, now=None):
        index = len(self.made)
        assert index < self.send_sem.shape[0]

        def make():
            return pltpu.make_async_remote_copy(
                src_ref=src(),
                dst_ref=dst(),
                send_sem=self.send_sem.at[index],
                recv_sem=recv_sem(),
                device_id=device,
                device_id_type=MESH,
            )

        self.made.append((make, cond))
        guarded(both_of(cond, now), lambda: make().start())

    def drain(self):
        for make, cond in self.made:
            guarded(cond, lambda make=make: make().wait_send())


def guarded(cond, act):
    if cond is None:
        act()
    else:
        pl.when(cond)(lambda: act())


def both_of(first, second):
    if first is None or second is None:
        return second if first is None else first
    return jnp.logical_and(first, second)


def rows_at(start, size):
    if isinstance(start, int):
        return pl.ds(start, size)
    return pl.ds(pl.multiple_of(start, size), size)


def send_count(n_z, chunks):
    mixer = 4 + 10 * (n_z - 1)
    weights = chunks + 1 + (chunks + pieces) * (2 * (n_z - 1) + 4)
    return mixer + weights + 9


def layer_kernel(
    n_z,
    tokens,
    mixer_gain,
    mix_w,
    taps,
    offset,
    recur_w,
    recur_b,
    input_w,
    input_b,
    logit,
    out_w,
    channel_gain,
    gate_w,
    up_w,
    gate_taps,
    gate_base,
    down_w,
    out,
    tok,
    mixb,
    outb,
    branch,
    recurrent,
    term_send,
    term_recv,
    term_own,
    residual,
    acts,
    gub,
    gub_swap,
    dnb,
    dnb_swap,
    hid,
    half_send,
    half_recv,
    half_own,
    chip_own,
    chip_send,
    chip_recv,
    result,
    local_sem,
    send_sem,
    mix_sem,
    gu_sem,
    dn_sem,
    term_sem,
    act_sem,
    half_send_sem,
    half_recv_sem,
    chip_send_sem,
    chip_recv_sem,
    out_send_sem,
    out_recv_sem,
    write_sem,
):
    x = lax.axis_index("rep")
    f = lax.axis_index("fs")
    t = lax.axis_index("tp")
    z, y = f // 2, f % 2
    n_f = 2 * n_z
    length, width = tokens.shape
    depth, channels = mix_w.shape
    chunks = gub.shape[0]
    units = chunks * unit_tile
    half = length // 2
    dim = recur_w.shape[1]

    def at(x_at, z_at, y_at, t_at):
        return (x_at, z_at * 2 + y_at, t_at)

    other_x, other_y, other_t = 1 - x, 1 - y, 1 - t
    near = {1: at(other_x, z, y, t), 2: at(x, z, other_y, t), 3: at(other_x, z, other_y, t)}
    partner = at(x, z, y, other_t)
    beside = z * 2 + other_y
    relay = n_z == 4
    toward = jnp.where(2 * z < n_z, 1, n_z - 1)
    column = [(z + step * (toward if relay else 1)) % n_z for step in range(n_z)]
    edge = n_z - 1
    is_mid = jnp.logical_and(z > 0, z < edge) if relay else None
    mid_from = column[1:3]
    mid_to = column[edge]
    mid_device = at(x, mid_to, y, t)

    def relayed(z_at):
        return jnp.logical_and(is_mid, z_at != mid_to)

    def direct(step):
        if not relay or step == 1:
            return None
        return jnp.logical_not(is_mid) if step == 2 else is_mid

    quarter = x * 2 + y
    quarter_swap = x * 2 + other_y
    local = []

    def bring(src, dst):
        copy = pltpu.make_async_copy(src, dst, local_sem.at[len(local)])
        copy.start()
        local.append(copy)
        return copy

    own_rows = rows_at(f * depth, depth)
    got_mix = [bring(mix_w, mixb.at[own_rows, :]), bring(out_w, outb.at[:, own_rows])]

    def unit_cols(which, chunk):
        return rows_at(which * units + chunk * unit_tile, unit_tile)

    low, high = pl.ds(0, unit_tile), pl.ds(unit_tile, unit_tile)
    got_own, got_swap = [], []
    for c in range(chunks):
        got_own.append(
            [
                bring(gate_w.at[:, unit_cols(quarter, c)], gub.at[c, own_rows, low]),
                bring(up_w.at[:, unit_cols(quarter, c)], gub.at[c, own_rows, high]),
            ]
        )
        got_swap.append(
            [
                bring(gate_w.at[:, unit_cols(quarter_swap, c)], gub_swap.at[c, :, low]),
                bring(up_w.at[:, unit_cols(quarter_swap, c)], gub_swap.at[c, :, high]),
            ]
        )
    got_tok = [bring(tokens, tok)]
    got_own.append([bring(down_w.at[rows_at(quarter * units, units), :], dnb.at[f])])
    got_swap.append([bring(down_w.at[rows_at(quarter_swap * units, units), :], dnb_swap)])

    barrier = pltpu.get_barrier_semaphore()
    peers = [near[1], near[2], near[3], partner] + [at(x, w, y, t) for w in column[1:]]
    for peer in peers:
        pl.semaphore_signal(barrier, inc=1, device_id=peer, device_id_type=MESH)
    pl.semaphore_wait(barrier, len(peers))

    copies = Copies(send_sem)

    def arrived(dst, sem, cond=None):
        def wait():
            copy = pltpu.make_async_remote_copy(
                src_ref=dst(),
                dst_ref=dst(),
                send_sem=sem(),
                recv_sem=sem(),
                device_id=partner,
                device_id_type=MESH,
            )
            copy.wait_recv()

        guarded(cond, wait)

    part_rows, part_out = depth // 2, channels // 2

    def mix_pieces(block, part):
        return [
            (
                lambda: mixb.at[rows_at(block * depth + part * part_rows, part_rows), :],
                lambda: mix_sem.at[block, 2 * part],
            ),
            (
                lambda: outb.at[rows_at(part * part_out, part_out), rows_at(block * depth, depth)],
                lambda: mix_sem.at[block, 2 * part + 1],
            ),
        ]

    def send_mix(block, part, device, cond=None):
        for ref, sem in mix_pieces(block, part):
            copies.send(ref, ref, sem, device, cond)

    def wait_mix(block, part):
        for ref, sem in mix_pieces(block, part):
            arrived(ref, sem)

    def weight_ref(stage, block):
        if stage == chunks:
            return lambda: dnb.at[block], lambda: dn_sem.at[block, 0]
        return lambda: gub.at[stage, rows_at(block * depth, depth), :], lambda: gu_sem.at[stage, block]

    def send_swap(stage):
        for copy in got_swap[stage]:
            copy.wait()
        ref, sem = weight_ref(stage, f)
        copies.send(lambda: dnb_swap if stage == chunks else gub_swap.at[stage], ref, sem, near[2])

    def send_block(stage, block, steps=range(1, n_z), also=None):
        ref, sem = weight_ref(stage, block)
        for step in steps:
            copies.send(ref, ref, sem, at(x, column[step], y, t), both_of(direct(step), also))

    def send_own(stage):
        for copy in got_own[stage]:
            copy.wait()
        send_block(stage, f)

    def send_first(inner):
        if not inner:
            for copy in got_own[0]:
                copy.wait()
            send_block(0, f, range(2 if relay else 1, n_z))
        if relay:
            send_block(0, f, range(1, 2), is_mid if inner else jnp.logical_not(is_mid))

    def send_beside(stage):
        arrived(*weight_ref(stage, beside))
        send_block(stage, beside)

    piece_width = depth // pieces

    def down_ref(block, piece):
        cols = rows_at(piece * piece_width, piece_width)
        return lambda: dnb.at[block, :, cols], lambda: dn_sem.at[block, piece]

    def send_down():
        for copy in got_own[chunks]:
            copy.wait()
        arrived(*weight_ref(chunks, beside))
        for side in range(2):
            for piece in range(pieces):
                ref, sem = down_ref(z * 2 + side, piece)
                for step in range(1, n_z):
                    copies.send(ref, ref, sem, at(x, column[step], y, t), direct(step))

    side_blocks = [[z_at * 2 + side for z_at in mid_from] for side in (y, other_y)]
    mid_blocks = [[z_at * 2 + side for side in range(2)] for z_at in mid_from]

    def relay_ref(ref, sem, now):
        arrived(ref, sem, both_of(is_mid, now))
        copies.send(ref, ref, sem, mid_device, is_mid, now)

    def relay_blocks(stage, blocks, now=None):
        if relay:
            for block in blocks:
                relay_ref(*weight_ref(stage, block), now)

    def relay_down(blocks, now=None):
        if relay:
            for block in blocks:
                for piece in range(pieces):
                    relay_ref(*down_ref(block, piece), now)

    def wait_stage(stage, now=None):
        for step in range(1, n_z):
            for side in (y, other_y):
                ref, sem = weight_ref(stage, column[step] * 2 + side)
                fresh = None
                if relay:
                    fresh = jnp.logical_not(is_mid) if step < edge else None
                arrived(ref, sem, both_of(fresh, now))

    for copy in got_mix:
        copy.wait()
    for step in range(1, n_z):
        send_mix(f, x, at(x, column[step], y, t), direct(step))
    for part in range(2):
        send_mix(f, part, near[2])
    send_first(False)
    send_swap(0)

    def norm_rows(source, gain, dest, total, size=64):
        def body(i, carry):
            at_rows = rows_at(i * size, size)
            widened = source[at_rows, :].astype(jnp.float32)
            scaled = widened * lax.rsqrt(jnp.mean(widened * widened, axis=-1, keepdims=True) + epsilon)
            dest[at_rows, :] = (scaled * gain[...]).astype(jnp.bfloat16)
            return carry

        lax.fori_loop(0, total // size, body, 0)

    for copy in got_tok:
        copy.wait()
    norm_rows(tok, mixer_gain, acts.at[0], length)

    order = range(1, n_z)
    for step in order:
        block = column[step] * 2 + y
        wait_mix(block, x)
        send_mix(block, x, near[2])
        send_mix(block, x, near[1])
        if relay and step < edge:
            send_mix(block, x, mid_device, is_mid)
    send_first(True)
    for stage in range(1, chunks + 1):
        send_swap(stage)
    send_beside(0)
    relay_blocks(0, side_blocks[0])
    send_own(1)
    for step in order:
        block = column[step] * 2 + other_y
        wait_mix(block, x)
        send_mix(block, x, near[1])
    relay_blocks(0, side_blocks[1])
    send_beside(1)
    for part in range(2):
        wait_mix(beside, part)
    for step in order:
        for side in (y, other_y):
            wait_mix(column[step] * 2 + side, other_x)
    def branch_body(j, carry):
        cols = rows_at(j * 256, 256)
        branch[:, cols] = (
            jnp.dot(acts[0], mixb[:, cols], preferred_element_type=jnp.float32).astype(jnp.bfloat16).astype(jnp.float32)
        )
        return carry

    lax.fori_loop(0, channels // 256, branch_body, 0)

    def block_body(k, carry):
        cols = rows_at(k * dim, dim)
        recurrent[:, cols] = recur_block(
            branch[:, cols],
            taps[:, cols],
            offset[:, cols],
            recur_w[k],
            recur_b[:, cols],
            input_w[k],
            input_b[:, cols],
            lru_scale * log_sigmoid(logit[:, cols]),
        )
        return carry

    lax.fori_loop(0, channels // dim, block_body, 0)

    relay_blocks(1, side_blocks[0])
    send_own(2)
    send_beside(2)

    def project(which, dest):
        rows = rows_at(which * half, half)

        def body(j, carry):
            cols = rows_at(j * 512, 512)
            dest[:, cols] = jnp.dot(recurrent[rows, :], outb[:, cols], preferred_element_type=jnp.float32).astype(
                jnp.bfloat16
            )
            return carry

        lax.fori_loop(0, width // 512, body, 0)

    project(other_t, term_send)
    copies.send(lambda: term_send, lambda: term_recv, lambda: term_sem.at[0], partner)
    project(t, term_own)
    arrived(lambda: term_recv, lambda: term_sem.at[0])
    mine = rows_at(t * half, half)
    theirs = rows_at(other_t * half, half)

    def residual_body(i, carry):
        rows = rows_at(i * 64, 64)
        total = term_own[rows, :].astype(jnp.float32) + term_recv[rows, :].astype(jnp.float32)
        base = tok[rows_at(t * half + i * 64, 64), :].astype(jnp.float32)
        residual[rows, :] = (base + total).astype(jnp.bfloat16)
        return carry

    lax.fori_loop(0, half // 64, residual_body, 0)
    norm_rows(residual, channel_gain, acts.at[0, mine, :], half)
    def act_part(slot, rows):
        return lambda: acts.at[slot, rows, :]

    def act_arrival(slot, hop):
        return lambda: act_sem.at[slot, hop]

    for slot in (1, 2, 3):
        copies.send(act_part(0, mine), act_part(slot, mine), act_arrival(slot, 0), near[slot])
    copies.send(act_part(0, mine), act_part(0, mine), act_arrival(0, 1), partner)
    relay_blocks(1, side_blocks[1])
    relay_blocks(2, side_blocks[0])
    relay_blocks(2, side_blocks[1])
    send_down()

    def pass_on(slot, now):
        arrived(act_part(slot, mine), act_arrival(slot, 0), now)
        copies.send(act_part(slot, mine), act_part(slot, mine), act_arrival(slot, 1), partner, None, now)

    def wait_acts(slot, now):
        arrived(act_part(slot, theirs), act_arrival(slot, 1), now)

    early = max(chunks - 1, 1)
    plan = [(slot, c) for slot in range(4) for c in range(early)]
    plan += [(slot, c) for c in range(early, chunks) for slot in range(4)]
    hooks = [[] for _ in plan]
    for number, (slot, c) in enumerate(plan):
        if slot == 0:
            hooks[number].append(functools.partial(wait_stage, c))
        if c == 0:
            hooks[number].append(functools.partial(wait_acts, slot))
    for slot in (1, 2, 3):
        hooks[slot * early - 1].append(functools.partial(pass_on, slot))

    rows_iota = lax.broadcasted_iota(jnp.int32, (length, unit_tile), 0)

    def gate_body(number, carry):
        late = number >= 4 * early
        slot = jnp.where(late, (number - 4 * early) % 4, number // early)
        c = jnp.where(late, early + (number - 4 * early) // 4, number % early)
        for index, acting in enumerate(hooks):
            for act in acting:
                act(now=number == index)

        both = jnp.dot(acts[slot], gub[c], preferred_element_type=jnp.float32)
        gate = both[:, :unit_tile].astype(jnp.bfloat16).astype(jnp.float32)
        up = both[:, unit_tile:].astype(jnp.bfloat16).astype(jnp.float32)
        cols = rows_at(quarter * units + c * unit_tile, unit_tile)
        width_taps = gate_taps.shape[0]
        mixed = gate_base[:, cols] + gate * gate_taps[width_taps - 1 : width_taps, cols]
        for back in range(1, width_taps):
            moved = jnp.where(rows_iota >= back, pltpu.roll(gate, back, 0), 0.0)
            mixed = mixed + moved * gate_taps[width_taps - 1 - back : width_taps - back, cols]
        hidden = (jax.nn.gelu(mixed) * up).astype(jnp.bfloat16)
        place = rows_at(c * unit_tile, unit_tile)
        rows = rows_at(slot * half, half)
        hid[0, rows, place] = hidden[:half]
        hid[1, rows, place] = hidden[half:]
        return carry

    lax.fori_loop(0, len(plan), gate_body, 0)
    relay_down(mid_blocks[0])

    n_b = n_f * pieces

    def block_of(i):
        k, side = i // (2 * pieces), (i // pieces) % 2
        if n_z == 4:
            return (((z // 2 + k // 2) % 2) * 2 + (z % 2 + k % 2) % 2) * 2 + side
        return ((z + k) % n_z) * 2 + side

    def cols_of(i):
        return rows_at((block_of(i) * pieces + i % pieces) * piece_width, piece_width)

    def half_copy(i):
        return pltpu.make_async_remote_copy(
            src_ref=half_send.at[i],
            dst_ref=half_recv.at[i],
            send_sem=half_send_sem.at[0],
            recv_sem=half_recv_sem.at[i],
            device_id=partner,
            device_id_type=MESH,
        )

    def chip_copy(i, slot):
        return pltpu.make_async_remote_copy(
            src_ref=chip_send.at[i, slot - 1],
            dst_ref=chip_recv.at[i, slot - 1],
            send_sem=chip_send_sem.at[0],
            recv_sem=chip_recv_sem.at[i],
            device_id=near[slot],
            device_id_type=MESH,
        )

    def out_copy(i):
        return pltpu.make_async_remote_copy(
            src_ref=result.at[:, cols_of(i)],
            dst_ref=out.at[mine, cols_of(i)],
            send_sem=out_send_sem.at[0],
            recv_sem=out_recv_sem.at[0],
            device_id=partner,
            device_id_type=MESH,
        )

    def write_copy(i):
        return pltpu.make_async_copy(result.at[:, cols_of(i)], out.at[mine, cols_of(i)], write_sem.at[0])

    lag = 3

    def down_body(i, carry):
        relay_down(mid_blocks[1], i == 2 * pieces)

        block, cols = block_of(i), rows_at((i % pieces) * piece_width, piece_width)
        fresh = jnp.logical_and(block != f, block != beside)
        if relay:
            fresh = jnp.logical_and(fresh, jnp.logical_not(relayed(block // 2)))
        arrived(lambda: dnb.at[block, :, cols], lambda: dn_sem.at[block, i % pieces], fresh)
        weight = dnb[block, :, cols]
        half_send[i] = jnp.dot(hid[other_t], weight, preferred_element_type=jnp.float32).astype(jnp.bfloat16)
        half_copy(i).start()
        half_own[...] = jnp.dot(hid[t], weight, preferred_element_type=jnp.float32).astype(jnp.bfloat16)
        half_copy(i).wait_recv()

        def add(slot):
            rows = pl.ds(slot * half, half)
            return half_own[rows, :].astype(jnp.float32) + half_recv[i, rows, :].astype(jnp.float32)

        before = None
        for slot in (3, 1, 2):
            chip_send[i, slot - 1] = add(slot).astype(jnp.bfloat16)
            if before is not None:
                chip_copy(i, before).start()
            before = slot
        chip_own[i] = add(0)
        chip_copy(i, before).start()

        pl.when(i >= lag)(lambda: finish(i - lag))
        return carry

    def finish(m):
        arrived(lambda: chip_recv.at[m], lambda: chip_recv_sem.at[m])
        total = chip_own[m]
        for slot in range(3):
            total = total + chip_recv[m, slot].astype(jnp.float32)
        result[:, cols_of(m)] = (residual[:, cols_of(m)].astype(jnp.float32) + total).astype(jnp.bfloat16)
        out_copy(m).start()
        write_copy(m).start()

    def finish_body(m, carry):
        finish(m)
        return carry

    lax.fori_loop(0, n_b, down_body, 0)
    copies.drain()
    lax.fori_loop(n_b - lag, n_b, finish_body, 0)

    def sent(ref, sem):
        pltpu.make_async_remote_copy(
            src_ref=ref, dst_ref=ref, send_sem=sem, recv_sem=sem, device_id=partner, device_id_type=MESH
        ).wait_send()

    sent(half_send, half_send_sem.at[0])
    sent(chip_send, chip_send_sem.at[0])
    sent(result, out_send_sem.at[0])
    pltpu.make_async_copy(result, out.at[mine, :], write_sem.at[0]).wait()
    arrived(lambda: out.at[theirs, :], lambda: out_recv_sem.at[0])


def log_sigmoid(v):
    small = jnp.exp(-jnp.abs(v))
    ratio = small / (2.0 + small)
    square = ratio * ratio
    series = 1.0 / 15.0
    for order in (13.0, 11.0, 9.0, 7.0, 5.0, 3.0, 1.0):
        series = 1.0 / order + square * series
    return jnp.minimum(v, 0.0) - 2.0 * ratio * series


def recur_block(branch, taps, offset, recur_weight, recur_bias, input_weight, input_bias, rate):
    length = branch.shape[0]
    width = taps.shape[0]
    rows = lax.broadcasted_iota(jnp.int32, branch.shape, 0)

    def shifted(values, step, fill):
        return jnp.where(rows >= step, pltpu.roll(values, step, 0), fill)

    total = offset + branch * taps[width - 1 : width, :]
    for back in range(1, width):
        total = total + shifted(branch, back, 0.0) * taps[width - 1 - back : width - back, :]
    smoothed = total.astype(jnp.bfloat16)
    recur = jnp.dot(smoothed, recur_weight, preferred_element_type=jnp.float32)
    recur_gate = jax.nn.sigmoid(recur + recur_bias)
    gated = jnp.dot(smoothed, input_weight, preferred_element_type=jnp.float32)
    input_gate = jax.nn.sigmoid(gated + input_bias)
    log_decay = recur_gate * rate
    state = jnp.sqrt(one_minus_exp(2.0 * log_decay)) * (input_gate * smoothed.astype(jnp.float32))
    decay = jnp.exp(log_decay)
    step = 1
    while step < length:
        state = state + decay * shifted(state, step, 0.0)
        if 2 * step < length:
            decay = decay * shifted(decay, step, 1.0)
        step *= 2
    return state.astype(jnp.bfloat16)


def fused(
    n_fs,
    tokens,
    mixer_gain,
    mix_weight,
    mixer_conv,
    mixer_offset,
    recur_weight,
    recur_bias,
    input_weight,
    input_bias,
    decay_logit,
    out_weight,
    channel_gain,
    gate_weight,
    up_weight,
    gate_conv,
    gate_offset,
    down_weight,
):
    n_z = n_fs // 2
    length, width = tokens.shape
    depth, channels = mix_weight.shape
    units = gate_weight.shape[1] // 4
    chunks = units // unit_tile
    half = length // 2
    n_b = n_fs * pieces
    row = lambda v: v.reshape(1, v.shape[0])
    hbm = pl.BlockSpec(memory_space=pl.ANY)
    vmem = pl.BlockSpec(memory_space=pltpu.VMEM)
    bf16, f32 = jnp.bfloat16, jnp.float32
    dma = pltpu.SemaphoreType.DMA
    rows_out = pl.pallas_call(
        functools.partial(layer_kernel, n_z),
        name="layer",
        in_specs=[hbm, vmem, hbm] + [vmem] * 7 + [hbm, vmem, hbm, hbm, vmem, vmem, hbm],
        out_specs=hbm,
        out_shape=jax.ShapeDtypeStruct((length, width), bf16),
        scratch_shapes=[
            pltpu.VMEM((length, width), bf16),
            pltpu.VMEM((width, channels), bf16),
            pltpu.VMEM((channels, width), bf16),
            pltpu.VMEM((length, channels), f32),
            pltpu.VMEM((length, channels), bf16),
            pltpu.VMEM((half, width), bf16),
            pltpu.VMEM((half, width), bf16),
            pltpu.VMEM((half, width), bf16),
            pltpu.VMEM((half, width), bf16),
            pltpu.VMEM((4, length, width), bf16),
            pltpu.VMEM((chunks, width, 2 * unit_tile), bf16),
            pltpu.VMEM((chunks, depth, 2 * unit_tile), bf16),
            pltpu.VMEM((n_fs, units, depth), bf16),
            pltpu.VMEM((units, depth), bf16),
            pltpu.VMEM((2, 4 * half, units), bf16),
            pltpu.VMEM((n_b, 4 * half, depth // pieces), bf16),
            pltpu.VMEM((n_b, 4 * half, depth // pieces), bf16),
            pltpu.VMEM((4 * half, depth // pieces), bf16),
            pltpu.VMEM((n_b, half, depth // pieces), f32),
            pltpu.VMEM((n_b, 3, half, depth // pieces), bf16),
            pltpu.VMEM((n_b, 3, half, depth // pieces), bf16),
            pltpu.VMEM((half, width), bf16),
            dma((5 + 4 * chunks,)),
            dma((send_count(n_z, chunks),)),
            dma((n_fs, 4)),
            dma((chunks, n_fs)),
            dma((n_fs, pieces)),
            dma((1,)),
            dma((4, 2)),
            dma((1,)),
            dma((n_b,)),
            dma((1,)),
            dma((n_b,)),
            dma((1,)),
            dma((1,)),
            dma((1,)),
        ],
        compiler_params=pltpu.CompilerParams(
            collective_id=0, has_side_effects=True, vmem_limit_bytes=56 * 2**20
        ),
    )(
        tokens,
        row(mixer_gain),
        mix_weight,
        mixer_conv,
        row(mixer_offset),
        recur_weight,
        row(recur_bias),
        input_weight,
        row(input_bias),
        row(decay_logit),
        out_weight,
        row(channel_gain),
        gate_weight,
        up_weight,
        gate_conv,
        row(gate_offset),
        down_weight,
    )
    parts = 4
    return pl.pallas_call(
        write_out,
        name="write_out",
        in_specs=[pl.BlockSpec(memory_space=pltpu.HBM)],
        out_specs=pl.BlockSpec(memory_space=pltpu.HBM),
        out_shape=jax.ShapeDtypeStruct((length, width), bf16),
        scratch_shapes=[pltpu.VMEM((parts, length // parts, width), bf16), dma((2, parts))],
        compiler_params=pltpu.CompilerParams(vmem_limit_bytes=62 * 2**20),
    )(rows_out)


def write_out(rows_ref, out_ref, held, sem):
    parts, size, _ = held.shape
    copies_in = [
        pltpu.make_async_copy(rows_ref.at[pl.ds(k * size, size), :], held.at[k], sem.at[0, k]) for k in range(parts)
    ]
    copies_out = [
        pltpu.make_async_copy(held.at[k], out_ref.at[pl.ds(k * size, size), :], sem.at[1, k]) for k in range(parts)
    ]
    for copy in copies_in:
        copy.start()
    for k in range(parts):
        copies_in[k].wait()
        copies_out[k].start()
    for copy in copies_out:
        copy.wait()


def local(n_rep, n_fs, n_tp, *arrays):
    units, columns = arrays[16].shape
    fits = n_rep == 2 and n_tp == 2 and n_fs % 2 == 0 and n_fs <= 8
    if fits and units == 12 * unit_tile and columns % 128 == 0:
        return fused(n_fs, *arrays)
    return plain(n_rep, n_fs, n_tp, *arrays)


def solution(mesh):
    in_specs = (
        P(("rep", "fs"), None),
        P(),
        P("fs", "tp"),
        P(None, "tp"),
        P("tp"),
        P("tp", None, None),
        P("tp"),
        P("tp", None, None),
        P("tp"),
        P("tp"),
        P("tp", "fs"),
        P(),
        P("fs", "tp"),
        P("fs", "tp"),
        P(None, "tp"),
        P("tp"),
        P("tp", "fs"),
    )
    out_specs = P(("rep", "fs"), None)
    body = functools.partial(local, mesh.shape["rep"], mesh.shape["fs"], mesh.shape["tp"])
    return jax.shard_map(body, mesh=mesh, in_specs=in_specs, out_specs=out_specs, check_vma=False)
```

```python
import functools
import itertools
import math

import jax
import jax.numpy as jnp
from jax import lax
from jax.experimental import pallas as pl
from jax.experimental.pallas import tpu as pltpu
from jax.sharding import PartitionSpec as P

epsilon = 1e-06
lru_scale = 8.0


def rms_rows(values, gain_row):
    widened = values.astype(jnp.float32)
    scaled = widened * lax.rsqrt(jnp.mean(widened * widened, axis=-1, keepdims=True) + epsilon)
    return (scaled * gain_row).astype(jnp.bfloat16)


def causal_conv(values, tap_rows, offset):
    width = tap_rows.shape[0]
    length = values.shape[-2]
    padding = [(0, 0)] * (values.ndim - 2) + [(width - 1, 0), (0, 0)]
    padded = jnp.pad(values, padding)
    total = offset + padded[..., 0:length, :] * tap_rows[0]
    for tap_index in range(1, width):
        total = total + padded[..., tap_index : tap_index + length, :] * tap_rows[tap_index]
    return total


def one_minus_exp(v):
    series = 1.0 + v * (1.0 / 7.0)
    for order in (6.0, 5.0, 4.0, 3.0, 2.0):
        series = 1.0 + v * (1.0 / order) * series
    return jnp.where(v > -0.25, -v * series, 1.0 - jnp.exp(v))


def mixer_kernel(
    branch_ref, taps_ref, offset_ref, recur_ref, recur_bias_ref, input_ref, input_bias_ref, rate_ref, out_ref
):
    branch = branch_ref[...].astype(jnp.float32)
    length = branch.shape[0]
    width = taps_ref.shape[0]
    rows = lax.broadcasted_iota(jnp.int32, branch.shape, 0)

    def shifted(values, step, fill):
        return jnp.where(rows >= step, pltpu.roll(values, step, 0), fill)

    total = offset_ref[...] + branch * taps_ref[width - 1 : width, :]
    for back in range(1, width):
        total = total + shifted(branch, back, 0.0) * taps_ref[width - 1 - back : width - back, :]
    smoothed = total.astype(jnp.bfloat16)
    recur = jnp.dot(smoothed, recur_ref[0], preferred_element_type=jnp.float32)
    recur_gate = jax.nn.sigmoid(recur + recur_bias_ref[...])
    gated = jnp.dot(smoothed, input_ref[0], preferred_element_type=jnp.float32)
    input_gate = jax.nn.sigmoid(gated + input_bias_ref[...])
    log_decay = recur_gate * rate_ref[...]
    state = jnp.sqrt(one_minus_exp(2.0 * log_decay)) * (input_gate * smoothed.astype(jnp.float32))
    decay = jnp.exp(log_decay)
    step = 1
    while step < length:
        state = state + decay * shifted(state, step, 0.0)
        if 2 * step < length:
            decay = decay * shifted(decay, step, 1.0)
        step *= 2
    out_ref[...] = state.astype(jnp.bfloat16)


def mixer(branch, taps, offset, recur_weight, recur_bias, input_weight, input_bias, rate):
    length, channels = branch.shape
    blocks, dim, _ = recur_weight.shape
    column = lambda rows: pl.BlockSpec((rows, dim), lambda k: (0, k))
    square = pl.BlockSpec((1, dim, dim), lambda k: (k, 0, 0))
    row = lambda v: v.reshape(1, channels)
    return pl.pallas_call(
        mixer_kernel,
        name="mixer",
        grid=(blocks,),
        in_specs=[
            column(length),
            column(taps.shape[0]),
            column(1),
            square,
            column(1),
            square,
            column(1),
            column(1),
        ],
        out_specs=column(length),
        out_shape=jax.ShapeDtypeStruct((length, channels), jnp.bfloat16),
        cost_estimate=pl.CostEstimate(
            flops=60 * length * channels + 4 * length * channels * dim,
            bytes_accessed=4 * length * channels,
            transcendentals=5 * length * channels,
        ),
    )(
        branch,
        taps,
        row(offset),
        recur_weight,
        row(recur_bias),
        input_weight,
        row(input_bias),
        row(rate),
    )


def shift(values, axis, count, step):
    return lax.ppermute(values, axis, [(i, (i + step) % count) for i in range(count)])


def take(values, index, size, axis=0):
    return lax.dynamic_slice_in_dim(values, index * size, size, axis)


def pair_gather(weight, count, axis):
    groups = [list(range(parity, count, 2)) for parity in range(2)]
    own = lax.all_gather(weight, "fs", axis=axis, axis_index_groups=groups, tiled=True)
    other = lax.ppermute(own, "fs", [(i, i ^ 1) for i in range(count)])
    return own, other


def pair_columns(values, count, parity):
    rows, width = values.shape
    size = width // count
    blocks = [values[:, i * size : (i + 1) * size] for i in range(count)]
    even = jnp.concatenate(blocks[0::2], axis=1)
    odd = jnp.concatenate(blocks[1::2], axis=1)
    return jnp.where(parity == 0, even, odd), jnp.where(parity == 0, odd, even)


def scatter_rows(partial, n_tp, me):
    size = partial.shape[0] // n_tp
    total = take(partial, me, size).astype(jnp.float32)
    for step in range(1, n_tp):
        sent = take(partial, lax.rem(me + step, n_tp), size)
        total = total + shift(sent, "tp", n_tp, step).astype(jnp.float32)
    return total


def collect_rows(share, n_tp, me):
    size = share.shape[0]
    if n_tp == 2:
        other = shift(share, "tp", n_tp, 1)
        first = jnp.where(me == 0, share, other)
        second = jnp.where(me == 0, other, share)
        return jnp.concatenate([first, second], axis=0)
    whole = jnp.zeros((size * n_tp, share.shape[1]), share.dtype)
    whole = lax.dynamic_update_slice_in_dim(whole, share, me * size, 0)
    for step in range(1, n_tp):
        got = shift(share, "tp", n_tp, step)
        whole = lax.dynamic_update_slice_in_dim(whole, got, lax.rem(me - step + n_tp, n_tp) * size, 0)
    return whole


def plain(
    n_rep,
    n_fs,
    n_tp,
    tokens,
    mixer_gain,
    mix_weight,
    mixer_conv,
    mixer_offset,
    recur_weight,
    recur_bias,
    input_weight,
    input_bias,
    decay_logit,
    out_weight,
    channel_gain,
    gate_weight,
    up_weight,
    gate_conv,
    gate_offset,
    down_weight,
):
    rep = lax.axis_index("rep")
    tp = lax.axis_index("tp")
    parity = lax.rem(lax.axis_index("fs"), 2)
    length = tokens.shape[0]
    units = gate_weight.shape[1] // n_rep

    both = jnp.concatenate([mix_weight, out_weight.T], axis=1)
    both_full = lax.all_gather(both, "fs", axis=0, tiled=True)
    channels = mix_weight.shape[1]
    mixer_full, out_full = both_full[:, :channels], both_full[:, channels:]
    gate_own, gate_other = pair_gather(take(gate_weight, rep, units, 1), n_fs, 0)
    up_own, up_other = pair_gather(take(up_weight, rep, units, 1), n_fs, 0)
    down_full = lax.all_gather(take(down_weight, rep, units, 0), "fs", axis=1, tiled=True)
    gate_taps = take(gate_conv, rep, units, 1)
    gate_base = take(gate_offset, rep, units, 0)

    normed = rms_rows(tokens, mixer_gain)
    branch = jnp.dot(normed, mixer_full, preferred_element_type=jnp.float32).astype(jnp.bfloat16)
    recurrent = mixer(
        branch,
        mixer_conv,
        mixer_offset,
        recur_weight,
        recur_bias,
        input_weight,
        input_bias,
        lru_scale * jax.nn.log_sigmoid(decay_logit),
    )
    mixer_term = lax.dot_general(
        recurrent, out_full, (((1,), (1,)), ((), ())), preferred_element_type=jnp.float32
    )
    mixer_share = scatter_rows(mixer_term.astype(jnp.bfloat16), n_tp, tp)
    rows = length // n_tp
    residual = (take(tokens, tp, rows).astype(jnp.float32) + mixer_share).astype(jnp.bfloat16)
    normed_share = rms_rows(residual, channel_gain)

    shares = [normed_share]
    for step in range(1, n_rep):
        shares.append(shift(normed_share, "rep", n_rep, step))

    def channel_mixer(share):
        rows_in = collect_rows(share, n_tp, tp)
        left, right = pair_columns(rows_in, n_fs, parity)
        gate_rows = jnp.dot(left, gate_own, preferred_element_type=jnp.float32)
        gate_rows = gate_rows + jnp.dot(right, gate_other, preferred_element_type=jnp.float32)
        up_rows = jnp.dot(left, up_own, preferred_element_type=jnp.float32)
        up_rows = up_rows + jnp.dot(right, up_other, preferred_element_type=jnp.float32)
        gate_rows = gate_rows.astype(jnp.bfloat16)
        up_rows = up_rows.astype(jnp.bfloat16)
        gate_mixed = causal_conv(gate_rows.astype(jnp.float32), gate_taps, gate_base)
        hidden = (jax.nn.gelu(gate_mixed) * up_rows.astype(jnp.float32)).astype(jnp.bfloat16)
        return jnp.dot(hidden, down_full, preferred_element_type=jnp.float32).astype(jnp.bfloat16)

    own_terms = channel_mixer(shares[0])
    total = None
    for step in range(1, n_rep):
        summed = scatter_rows(channel_mixer(shares[step]), n_tp, tp).astype(jnp.bfloat16)
        back = shift(summed, "rep", n_rep, -step).astype(jnp.float32)
        total = back if total is None else total + back
    own = scatter_rows(own_terms, n_tp, tp)
    total = own if total is None else own + total
    result = (residual.astype(jnp.float32) + total).astype(jnp.bfloat16)
    return collect_rows(result, n_tp, tp)


MESH = pl.DeviceIdType.MESH
unit_tile = 256
pieces = 2


class Copies:
    def __init__(self, send_sem, is_mid):
        self.send_sem = send_sem
        self.conds = {"all": None, "mid": is_mid, "end": jnp.logical_not(is_mid)}
        self.sizes = [{"all": 0, "mid": 0, "end": 0} for _ in range(send_sem.shape[0])]

    def send(self, src, dst, recv_sem, device, group, kind="all", now=None):
        def start():
            copy = pltpu.make_async_remote_copy(
                src_ref=src(),
                dst_ref=dst(),
                send_sem=self.send_sem.at[group],
                recv_sem=recv_sem(),
                device_id=device,
                device_id_type=MESH,
            )
            copy.start()

        self.sizes[group][kind] += size_of(src())
        guarded(both_of(self.conds[kind], now), start)

    def drain(self, spans, device):
        for group, size in enumerate(self.sizes):
            for kind in ("all",) if size["mid"] == size["end"] else ("mid", "end"):
                total = size["all"] + size["mid" if kind == "all" else kind]

                def wait(total=total, group=group):
                    wait_sent(span_of(spans, total), self.send_sem.at[group], device)

                guarded(self.conds[kind], wait)


def size_of(ref):
    return math.prod(ref.shape) * 2


def span_of(spans, total):
    for ref in spans:
        count, rows, columns = ref.shape
        need = total // (2 * columns)
        lots = -(-need // rows)
        if lots <= count and need % lots == 0:
            return ref.at[pl.ds(0, lots), pl.ds(0, need // lots), :]
    raise ValueError("no span")


def wait_sent(ref, sem, device):
    pltpu.make_async_remote_copy(
        src_ref=ref, dst_ref=ref, send_sem=sem, recv_sem=sem, device_id=device, device_id_type=MESH
    ).wait_send()


def guarded(cond, act):
    if cond is None:
        act()
    else:
        pl.when(cond)(lambda: act())


def both_of(first, second):
    if first is None or second is None:
        return second if first is None else first
    return jnp.logical_and(first, second)


def rows_at(start, size):
    if isinstance(start, int):
        return pl.ds(start, size)
    return pl.ds(pl.multiple_of(start, size), size)


def layer_kernel(
    n_z,
    tokens,
    mixer_gain,
    mix_w,
    taps,
    offset,
    recur_w,
    recur_b,
    input_w,
    input_b,
    logit,
    out_w,
    channel_gain,
    gate_w,
    up_w,
    gate_taps,
    gate_base,
    down_w,
    out,
    tok,
    mixb,
    outb,
    branch,
    recurrent,
    term_send,
    term_recv,
    term_own,
    residual,
    acts,
    gub,
    gub_swap,
    dnb,
    dnb_swap,
    hid,
    half_send,
    half_recv,
    half_own,
    chip_own,
    chip_send,
    chip_recv,
    local_sem,
    send_sem,
    mix_sem,
    gu_sem,
    dn_sem,
    term_sem,
    act_sem,
    half_send_sem,
    half_recv_sem,
    chip_send_sem,
    chip_recv_sem,
    out_send_sem,
    out_recv_sem,
):
    x = lax.axis_index("rep")
    f = lax.axis_index("fs")
    t = lax.axis_index("tp")
    z, y = f // 2, f % 2
    n_f = 2 * n_z
    length, width = tokens.shape
    depth, channels = mix_w.shape
    chunks = gub.shape[0]
    units = chunks * unit_tile
    half = length // 2
    dim = recur_w.shape[1]

    def at(x_at, z_at, y_at, t_at):
        return (x_at, z_at * 2 + y_at, t_at)

    other_x, other_y, other_t = 1 - x, 1 - y, 1 - t
    near = {1: at(other_x, z, y, t), 2: at(x, z, other_y, t), 3: at(other_x, z, other_y, t)}
    partner = at(x, z, y, other_t)
    beside = z * 2 + other_y
    toward = jnp.where(2 * z < n_z, 1, n_z - 1)
    column = [(z + step * toward) % n_z for step in range(n_z)]
    edge = n_z - 1
    is_mid = jnp.logical_and(z > 0, z < edge)
    mid_from = column[1:3]
    mid_to = column[edge]
    mid_device = at(x, mid_to, y, t)

    def relayed(z_at):
        return jnp.logical_and(is_mid, z_at != mid_to)

    def direct(step):
        return ("all", "end", "mid")[step - 1]

    barrier = pltpu.get_barrier_semaphore()
    peers = [near[1], near[2], near[3], partner] + [at(x, w, y, t) for w in column[1:]]
    for peer in peers:
        pl.semaphore_signal(barrier, inc=1, device_id=peer, device_id_type=MESH)

    quarter = x * 2 + y
    quarter_swap = x * 2 + other_y
    numbers = itertools.count()

    def bring(whole, *pairs):
        sem = local_sem.at[next(numbers)]
        for src, dst in pairs:
            pltpu.make_async_copy(src, dst, sem).start()
        return pltpu.make_async_copy(whole, whole, sem)

    own_rows = rows_at(f * depth, depth)
    both_blocks = mixb.at[pl.ds(0, 2 * depth), :]
    got_mix = bring(both_blocks, (mix_w, mixb.at[own_rows, :]), (out_w, outb.at[:, own_rows]))

    def unit_cols(which, chunk):
        return rows_at(which * units + chunk * unit_tile, unit_tile)

    low, high = pl.ds(0, unit_tile), pl.ds(unit_tile, unit_tile)
    got_own, got_swap = [], []
    for c in range(chunks):
        got_own.append(
            bring(
                gub.at[c, own_rows, :],
                (gate_w.at[:, unit_cols(quarter, c)], gub.at[c, own_rows, low]),
                (up_w.at[:, unit_cols(quarter, c)], gub.at[c, own_rows, high]),
            )
        )
        got_swap.append(
            bring(
                gub_swap.at[c],
                (gate_w.at[:, unit_cols(quarter_swap, c)], gub_swap.at[c, :, low]),
                (up_w.at[:, unit_cols(quarter_swap, c)], gub_swap.at[c, :, high]),
            )
        )
    got_tok = bring(tok, (tokens, tok))
    got_own.append(bring(dnb.at[f], (down_w.at[rows_at(quarter * units, units), :], dnb.at[f])))
    got_swap.append(bring(dnb_swap, (down_w.at[rows_at(quarter_swap * units, units), :], dnb_swap)))

    pl.semaphore_wait(barrier, len(peers))

    copies = Copies(send_sem, is_mid)
    mix_group, swap_group, down_group, act_group = range(chunks, chunks + 4)

    def arrived(dst, sem, cond=None):
        def wait():
            copy = pltpu.make_async_remote_copy(
                src_ref=dst(),
                dst_ref=dst(),
                send_sem=sem(),
                recv_sem=sem(),
                device_id=partner,
                device_id_type=MESH,
            )
            copy.wait_recv()

        guarded(cond, wait)

    part_rows, part_out = depth // 2, channels // 2

    def mix_pieces(block, part):
        return [
            (
                lambda: mixb.at[rows_at(block * depth + part * part_rows, part_rows), :],
                lambda: mix_sem.at[block, part],
            ),
            (
                lambda: outb.at[rows_at(part * part_out, part_out), rows_at(block * depth, depth)],
                lambda: mix_sem.at[block, part],
            ),
        ]

    def send_mix(block, part, device, kind="all"):
        for ref, sem in mix_pieces(block, part):
            copies.send(ref, ref, sem, device, mix_group, kind)

    def wait_mix(block, part):
        arrived(lambda: mixb.at[rows_at(block * depth, depth), :], lambda: mix_sem.at[block, part])

    def weight_ref(stage, block):
        if stage == chunks:
            return lambda: dnb.at[block], lambda: dn_sem.at[block, 0]
        return lambda: gub.at[stage, rows_at(block * depth, depth), :], lambda: gu_sem.at[stage, block]

    def send_swap(stage):
        got_swap[stage].wait()
        ref, sem = weight_ref(stage, f)
        copies.send(lambda: dnb_swap if stage == chunks else gub_swap.at[stage], ref, sem, near[2], swap_group)

    def send_block(stage, block, steps=range(1, n_z), kind=None):
        ref, sem = weight_ref(stage, block)
        for step in steps:
            copies.send(ref, ref, sem, at(x, column[step], y, t), stage, kind or direct(step))

    def send_own(stage):
        got_own[stage].wait()
        send_block(stage, f)

    def send_first(inner):
        if not inner:
            got_own[0].wait()
            send_block(0, f, range(2, n_z))
        send_block(0, f, range(1, 2), "mid" if inner else "end")

    def send_beside(stage):
        arrived(*weight_ref(stage, beside))
        send_block(stage, beside)

    piece_width = depth // pieces

    def down_ref(block, piece):
        cols = rows_at(piece * piece_width, piece_width)
        return lambda: dnb.at[block, :, cols], lambda: dn_sem.at[block, piece]

    def send_down():
        got_own[chunks].wait()
        arrived(*weight_ref(chunks, beside))
        for side in range(2):
            for piece in range(pieces):
                ref, sem = down_ref(z * 2 + side, piece)
                for step in range(1, n_z):
                    copies.send(ref, ref, sem, at(x, column[step], y, t), down_group, direct(step))

    side_blocks = [[z_at * 2 + side for z_at in mid_from] for side in (y, other_y)]
    mid_blocks = [[z_at * 2 + side for side in range(2)] for z_at in mid_from]

    def relay_ref(ref, sem, group, now):
        arrived(ref, sem, both_of(is_mid, now))
        copies.send(ref, ref, sem, mid_device, group, "mid", now)

    def relay_blocks(stage, blocks, now=None):
        for block in blocks:
            relay_ref(*weight_ref(stage, block), stage, now)

    def relay_down(blocks, now=None):
        for block in blocks:
            for piece in range(pieces):
                relay_ref(*down_ref(block, piece), down_group, now)

    def wait_stage(stage, now=None):
        for step in range(1, n_z):
            for side in (y, other_y):
                ref, sem = weight_ref(stage, column[step] * 2 + side)
                fresh = jnp.logical_not(is_mid) if step < edge else None
                arrived(ref, sem, both_of(fresh, now))

    got_mix.wait()
    for step in range(1, n_z):
        send_mix(f, x, at(x, column[step], y, t), direct(step))
    for part in range(2):
        send_mix(f, part, near[2])
    send_first(False)
    send_swap(0)

    def norm_rows(source, gain, dest, total, size=64):
        def body(i, carry):
            at_rows = rows_at(i * size, size)
            widened = source[at_rows, :].astype(jnp.float32)
            scaled = widened * lax.rsqrt(jnp.mean(widened * widened, axis=-1, keepdims=True) + epsilon)
            dest[at_rows, :] = (scaled * gain[...]).astype(jnp.bfloat16)
            return carry

        lax.fori_loop(0, total // size, body, 0)

    got_tok.wait()
    norm_rows(tok, mixer_gain, acts.at[0], length)

    order = range(1, n_z)
    for step in order:
        block = column[step] * 2 + y
        wait_mix(block, x)
        send_mix(block, x, near[2])
        send_mix(block, x, near[1])
        if step < edge:
            send_mix(block, x, mid_device, "mid")
    send_first(True)
    for stage in range(1, chunks + 1):
        send_swap(stage)
    send_beside(0)
    relay_blocks(0, side_blocks[0])
    send_own(1)
    for step in order:
        block = column[step] * 2 + other_y
        wait_mix(block, x)
        send_mix(block, x, near[1])
    relay_blocks(0, side_blocks[1])
    send_beside(1)
    for part in range(2):
        wait_mix(beside, part)
    for step in order:
        for side in (y, other_y):
            wait_mix(column[step] * 2 + side, other_x)
    def branch_body(j, carry):
        cols = rows_at(j * 256, 256)
        branch[:, cols] = (
            jnp.dot(acts[0], mixb[:, cols], preferred_element_type=jnp.float32).astype(jnp.bfloat16).astype(jnp.float32)
        )
        return carry

    lax.fori_loop(0, channels // 256, branch_body, 0)

    def block_body(k, carry):
        cols = rows_at(k * dim, dim)
        recurrent[:, cols] = recur_block(
            branch[:, cols],
            taps[:, cols],
            offset[:, cols],
            recur_w[k],
            recur_b[:, cols],
            input_w[k],
            input_b[:, cols],
            lru_scale * log_sigmoid(logit[:, cols]),
        )
        return carry

    lax.fori_loop(0, channels // dim, block_body, 0)

    relay_blocks(1, side_blocks[0])
    send_own(2)
    send_beside(2)

    def project(which, dest):
        rows = rows_at(which * half, half)

        def body(j, carry):
            cols = rows_at(j * 512, 512)
            dest[:, cols] = jnp.dot(recurrent[rows, :], outb[:, cols], preferred_element_type=jnp.float32).astype(
                jnp.bfloat16
            )
            return carry

        lax.fori_loop(0, width // 512, body, 0)

    project(other_t, term_send)
    copies.send(lambda: term_send, lambda: term_recv, lambda: term_sem.at[0], partner, act_group)
    project(t, term_own)
    arrived(lambda: term_recv, lambda: term_sem.at[0])
    mine = rows_at(t * half, half)
    theirs = rows_at(other_t * half, half)

    def residual_body(i, carry):
        rows = rows_at(i * 64, 64)
        total = term_own[rows, :].astype(jnp.float32) + term_recv[rows, :].astype(jnp.float32)
        base = tok[rows_at(t * half + i * 64, 64), :].astype(jnp.float32)
        residual[rows, :] = (base + total).astype(jnp.bfloat16)
        return carry

    lax.fori_loop(0, half // 64, residual_body, 0)
    norm_rows(residual, channel_gain, acts.at[0, mine, :], half)
    def act_part(slot, rows):
        return lambda: acts.at[slot, rows, :]

    def act_arrival(slot, hop):
        return lambda: act_sem.at[slot, hop]

    for slot in (1, 2, 3):
        copies.send(act_part(0, mine), act_part(slot, mine), act_arrival(slot, 0), near[slot], act_group)
    copies.send(act_part(0, mine), act_part(0, mine), act_arrival(0, 1), partner, act_group)
    relay_blocks(1, side_blocks[1])
    relay_blocks(2, side_blocks[0])
    relay_blocks(2, side_blocks[1])
    send_down()

    def pass_on(slot, now):
        arrived(act_part(slot, mine), act_arrival(slot, 0), now)
        copies.send(act_part(slot, mine), act_part(slot, mine), act_arrival(slot, 1), partner, act_group, now=now)

    def wait_acts(slot, now):
        arrived(act_part(slot, theirs), act_arrival(slot, 1), now)

    early = max(chunks - 1, 1)
    plan = [(slot, c) for slot in range(4) for c in range(early)]
    plan += [(slot, c) for c in range(early, chunks) for slot in range(4)]
    hooks = [[] for _ in plan]
    for number, (slot, c) in enumerate(plan):
        if slot == 0:
            hooks[number].append(functools.partial(wait_stage, c))
        if c == 0:
            hooks[number].append(functools.partial(wait_acts, slot))
    for slot in (1, 2, 3):
        hooks[slot * early - 1].append(functools.partial(pass_on, slot))

    rows_iota = lax.broadcasted_iota(jnp.int32, (length, unit_tile), 0)

    def gate_body(number, carry):
        late = number >= 4 * early
        slot = jnp.where(late, (number - 4 * early) % 4, number // early)
        c = jnp.where(late, early + (number - 4 * early) // 4, number % early)
        for index, acting in enumerate(hooks):
            for act in acting:
                act(now=number == index)

        both = jnp.dot(acts[slot], gub[c], preferred_element_type=jnp.float32)
        gate = both[:, :unit_tile].astype(jnp.bfloat16).astype(jnp.float32)
        up = both[:, unit_tile:].astype(jnp.bfloat16).astype(jnp.float32)
        cols = rows_at(quarter * units + c * unit_tile, unit_tile)
        width_taps = gate_taps.shape[0]
        mixed = gate_base[:, cols] + gate * gate_taps[width_taps - 1 : width_taps, cols]
        for back in range(1, width_taps):
            moved = jnp.where(rows_iota >= back, pltpu.roll(gate, back, 0), 0.0)
            mixed = mixed + moved * gate_taps[width_taps - 1 - back : width_taps - back, cols]
        hidden = (jax.nn.gelu(mixed) * up).astype(jnp.bfloat16)
        place = rows_at(c * unit_tile, unit_tile)
        rows = rows_at(slot * half, half)
        hid[0, rows, place] = hidden[:half]
        hid[1, rows, place] = hidden[half:]
        return carry

    lax.fori_loop(0, len(plan), gate_body, 0)
    relay_down(mid_blocks[0])

    n_b = n_f * pieces

    def block_of(i):
        k, side = i // (2 * pieces), (i // pieces) % 2
        return (((z // 2 + k // 2) % 2) * 2 + (z % 2 + k % 2) % 2) * 2 + side

    def cols_of(i):
        return rows_at((block_of(i) * pieces + i % pieces) * piece_width, piece_width)

    def half_copy(i):
        return pltpu.make_async_remote_copy(
            src_ref=half_send.at[i],
            dst_ref=half_recv.at[i],
            send_sem=half_send_sem.at[0],
            recv_sem=half_recv_sem.at[i],
            device_id=partner,
            device_id_type=MESH,
        )

    def chip_copy(i, slot):
        return pltpu.make_async_remote_copy(
            src_ref=chip_send.at[i, slot - 1],
            dst_ref=chip_recv.at[i, slot - 1],
            send_sem=chip_send_sem.at[0],
            recv_sem=chip_recv_sem.at[i],
            device_id=near[slot],
            device_id_type=MESH,
        )

    def out_copy(i):
        return pltpu.make_async_remote_copy(
            src_ref=out.at[mine, cols_of(i)],
            dst_ref=out.at[mine, cols_of(i)],
            send_sem=out_send_sem.at[0],
            recv_sem=out_recv_sem.at[0],
            device_id=partner,
            device_id_type=MESH,
        )

    lag = 3

    def down_body(i, carry):
        relay_down(mid_blocks[1], i == 2 * pieces)

        block, cols = block_of(i), rows_at((i % pieces) * piece_width, piece_width)
        fresh = jnp.logical_and(block != f, block != beside)
        fresh = jnp.logical_and(fresh, jnp.logical_not(relayed(block // 2)))
        arrived(lambda: dnb.at[block, :, cols], lambda: dn_sem.at[block, i % pieces], fresh)
        weight = dnb[block, :, cols]
        half_send[i] = jnp.dot(hid[other_t], weight, preferred_element_type=jnp.float32).astype(jnp.bfloat16)
        half_copy(i).start()
        half_own[...] = jnp.dot(hid[t], weight, preferred_element_type=jnp.float32).astype(jnp.bfloat16)
        half_copy(i).wait_recv()

        def add(slot):
            rows = pl.ds(slot * half, half)
            return half_own[rows, :].astype(jnp.float32) + half_recv[i, rows, :].astype(jnp.float32)

        before = None
        for slot in (3, 1, 2):
            chip_send[i, slot - 1] = add(slot).astype(jnp.bfloat16)
            if before is not None:
                chip_copy(i, before).start()
            before = slot
        chip_own[i] = add(0)
        chip_copy(i, before).start()

        pl.when(i >= lag)(lambda: finish(i - lag))
        return carry

    def finish(m):
        arrived(lambda: chip_recv.at[m], lambda: chip_recv_sem.at[m])
        total = chip_own[m]
        for slot in range(3):
            total = total + chip_recv[m, slot].astype(jnp.float32)
        out[mine, cols_of(m)] = (residual[:, cols_of(m)].astype(jnp.float32) + total).astype(jnp.bfloat16)
        out_copy(m).start()

    def finish_body(m, carry):
        finish(m)
        return carry

    lax.fori_loop(0, n_b, down_body, 0)
    copies.drain((gub, acts), partner)
    lax.fori_loop(n_b - lag, n_b, finish_body, 0)

    wait_sent(half_send, half_send_sem.at[0], partner)
    wait_sent(chip_send, chip_send_sem.at[0], partner)
    wait_sent(out.at[mine, :], out_send_sem.at[0], partner)
    arrived(lambda: out.at[theirs, :], lambda: out_recv_sem.at[0])


def log_sigmoid(v):
    small = jnp.exp(-jnp.abs(v))
    ratio = small / (2.0 + small)
    square = ratio * ratio
    series = 1.0 / 15.0
    for order in (13.0, 11.0, 9.0, 7.0, 5.0, 3.0, 1.0):
        series = 1.0 / order + square * series
    return jnp.minimum(v, 0.0) - 2.0 * ratio * series


def recur_block(branch, taps, offset, recur_weight, recur_bias, input_weight, input_bias, rate):
    length = branch.shape[0]
    width = taps.shape[0]
    rows = lax.broadcasted_iota(jnp.int32, branch.shape, 0)

    def shifted(values, step, fill):
        return jnp.where(rows >= step, pltpu.roll(values, step, 0), fill)

    total = offset + branch * taps[width - 1 : width, :]
    for back in range(1, width):
        total = total + shifted(branch, back, 0.0) * taps[width - 1 - back : width - back, :]
    smoothed = total.astype(jnp.bfloat16)
    recur = jnp.dot(smoothed, recur_weight, preferred_element_type=jnp.float32)
    recur_gate = jax.nn.sigmoid(recur + recur_bias)
    gated = jnp.dot(smoothed, input_weight, preferred_element_type=jnp.float32)
    input_gate = jax.nn.sigmoid(gated + input_bias)
    log_decay = recur_gate * rate
    state = jnp.sqrt(one_minus_exp(2.0 * log_decay)) * (input_gate * smoothed.astype(jnp.float32))
    decay = jnp.exp(log_decay)
    step = 1
    while step < length:
        state = state + decay * shifted(state, step, 0.0)
        if 2 * step < length:
            decay = decay * shifted(decay, step, 1.0)
        step *= 2
    return state.astype(jnp.bfloat16)


def fused(
    n_fs,
    tokens,
    mixer_gain,
    mix_weight,
    mixer_conv,
    mixer_offset,
    recur_weight,
    recur_bias,
    input_weight,
    input_bias,
    decay_logit,
    out_weight,
    channel_gain,
    gate_weight,
    up_weight,
    gate_conv,
    gate_offset,
    down_weight,
):
    n_z = n_fs // 2
    length, width = tokens.shape
    depth, channels = mix_weight.shape
    units = gate_weight.shape[1] // 4
    chunks = units // unit_tile
    half = length // 2
    n_b = n_fs * pieces
    row = lambda v: v.reshape(1, v.shape[0])
    hbm = pl.BlockSpec(memory_space=pl.ANY)
    vmem = pl.BlockSpec(memory_space=pltpu.VMEM)
    bf16, f32 = jnp.bfloat16, jnp.float32
    dma = pltpu.SemaphoreType.DMA
    rows_out = pl.pallas_call(
        functools.partial(layer_kernel, n_z),
        name="layer",
        in_specs=[hbm, vmem, hbm] + [vmem] * 7 + [hbm, vmem, hbm, hbm, vmem, vmem, hbm],
        out_specs=vmem,
        out_shape=pltpu.VMEM((length, width), bf16),
        scratch_shapes=[
            pltpu.VMEM((length, width), bf16),
            pltpu.VMEM((width, channels), bf16),
            pltpu.VMEM((channels, width), bf16),
            pltpu.VMEM((length, channels), f32),
            pltpu.VMEM((length, channels), bf16),
            pltpu.VMEM((half, width), bf16),
            pltpu.VMEM((half, width), bf16),
            pltpu.VMEM((half, width), bf16),
            pltpu.VMEM((half, width), bf16),
            pltpu.VMEM((4, length, width), bf16),
            pltpu.VMEM((chunks, width, 2 * unit_tile), bf16),
            pltpu.VMEM((chunks, depth, 2 * unit_tile), bf16),
            pltpu.VMEM((n_fs, units, depth), bf16),
            pltpu.VMEM((units, depth), bf16),
            pltpu.VMEM((2, 4 * half, units), bf16),
            pltpu.VMEM((n_b, 4 * half, depth // pieces), bf16),
            pltpu.VMEM((n_b, 4 * half, depth // pieces), bf16),
            pltpu.VMEM((4 * half, depth // pieces), bf16),
            pltpu.VMEM((n_b, half, depth // pieces), f32),
            pltpu.VMEM((n_b, 3, half, depth // pieces), bf16),
            pltpu.VMEM((n_b, 3, half, depth // pieces), bf16),
            dma((4 + 2 * chunks,)),
            dma((chunks + 4,)),
            dma((n_fs, 2)),
            dma((chunks, n_fs)),
            dma((n_fs, pieces)),
            dma((1,)),
            dma((4, 2)),
            dma((1,)),
            dma((n_b,)),
            dma((1,)),
            dma((n_b,)),
            dma((1,)),
            dma((1,)),
        ],
        compiler_params=pltpu.CompilerParams(
            collective_id=0, has_side_effects=True, vmem_limit_bytes=56 * 2**20
        ),
    )(
        tokens,
        row(mixer_gain),
        mix_weight,
        mixer_conv,
        row(mixer_offset),
        recur_weight,
        row(recur_bias),
        input_weight,
        row(input_bias),
        row(decay_logit),
        out_weight,
        row(channel_gain),
        gate_weight,
        up_weight,
        gate_conv,
        row(gate_offset),
        down_weight,
    )
    return rows_out


def local(n_rep, n_fs, n_tp, *arrays):
    units, columns = arrays[16].shape
    fits = n_rep == 2 and n_tp == 2 and n_fs == 8
    if fits and units == 12 * unit_tile and columns % 128 == 0:
        return fused(n_fs, *arrays)
    return plain(n_rep, n_fs, n_tp, *arrays)


def solution(mesh):
    in_specs = (
        P(("rep", "fs"), None),
        P(),
        P("fs", "tp"),
        P(None, "tp"),
        P("tp"),
        P("tp", None, None),
        P("tp"),
        P("tp", None, None),
        P("tp"),
        P("tp"),
        P("tp", "fs"),
        P(),
        P("fs", "tp"),
        P("fs", "tp"),
        P(None, "tp"),
        P("tp"),
        P("tp", "fs"),
    )
    out_specs = P(("rep", "fs"), None)
    body = functools.partial(local, mesh.shape["rep"], mesh.shape["fs"], mesh.shape["tp"])
    return jax.shard_map(body, mesh=mesh, in_specs=in_specs, out_specs=out_specs, check_vma=False)
```

```python
import functools
import itertools
import math

import jax
import jax.numpy as jnp
from jax import lax
from jax.experimental import pallas as pl
from jax.experimental.pallas import tpu as pltpu
from jax.sharding import PartitionSpec as P

epsilon = 1e-06
lru_scale = 8.0


def rms_rows(values, gain_row):
    widened = values.astype(jnp.float32)
    scaled = widened * lax.rsqrt(jnp.mean(widened * widened, axis=-1, keepdims=True) + epsilon)
    return (scaled * gain_row).astype(jnp.bfloat16)


def causal_conv(values, tap_rows, offset):
    width = tap_rows.shape[0]
    length = values.shape[-2]
    padding = [(0, 0)] * (values.ndim - 2) + [(width - 1, 0), (0, 0)]
    padded = jnp.pad(values, padding)
    total = offset + padded[..., 0:length, :] * tap_rows[0]
    for tap_index in range(1, width):
        total = total + padded[..., tap_index : tap_index + length, :] * tap_rows[tap_index]
    return total


def one_minus_exp(v):
    series = 1.0 + v * (1.0 / 7.0)
    for order in (6.0, 5.0, 4.0, 3.0, 2.0):
        series = 1.0 + v * (1.0 / order) * series
    return jnp.where(v > -0.25, -v * series, 1.0 - jnp.exp(v))


def mixer_kernel(
    branch_ref, taps_ref, offset_ref, recur_ref, recur_bias_ref, input_ref, input_bias_ref, rate_ref, out_ref
):
    branch = branch_ref[...].astype(jnp.float32)
    length = branch.shape[0]
    width = taps_ref.shape[0]
    rows = lax.broadcasted_iota(jnp.int32, branch.shape, 0)

    def shifted(values, step, fill):
        return jnp.where(rows >= step, pltpu.roll(values, step, 0), fill)

    total = offset_ref[...] + branch * taps_ref[width - 1 : width, :]
    for back in range(1, width):
        total = total + shifted(branch, back, 0.0) * taps_ref[width - 1 - back : width - back, :]
    smoothed = total.astype(jnp.bfloat16)
    recur = jnp.dot(smoothed, recur_ref[0], preferred_element_type=jnp.float32)
    recur_gate = jax.nn.sigmoid(recur + recur_bias_ref[...])
    gated = jnp.dot(smoothed, input_ref[0], preferred_element_type=jnp.float32)
    input_gate = jax.nn.sigmoid(gated + input_bias_ref[...])
    log_decay = recur_gate * rate_ref[...]
    state = jnp.sqrt(one_minus_exp(2.0 * log_decay)) * (input_gate * smoothed.astype(jnp.float32))
    decay = jnp.exp(log_decay)
    step = 1
    while step < length:
        state = state + decay * shifted(state, step, 0.0)
        if 2 * step < length:
            decay = decay * shifted(decay, step, 1.0)
        step *= 2
    out_ref[...] = state.astype(jnp.bfloat16)


def mixer(branch, taps, offset, recur_weight, recur_bias, input_weight, input_bias, rate):
    length, channels = branch.shape
    blocks, dim, _ = recur_weight.shape
    column = lambda rows: pl.BlockSpec((rows, dim), lambda k: (0, k))
    square = pl.BlockSpec((1, dim, dim), lambda k: (k, 0, 0))
    row = lambda v: v.reshape(1, channels)
    return pl.pallas_call(
        mixer_kernel,
        name="mixer",
        grid=(blocks,),
        in_specs=[
            column(length),
            column(taps.shape[0]),
            column(1),
            square,
            column(1),
            square,
            column(1),
            column(1),
        ],
        out_specs=column(length),
        out_shape=jax.ShapeDtypeStruct((length, channels), jnp.bfloat16),
        cost_estimate=pl.CostEstimate(
            flops=60 * length * channels + 4 * length * channels * dim,
            bytes_accessed=4 * length * channels,
            transcendentals=5 * length * channels,
        ),
    )(
        branch,
        taps,
        row(offset),
        recur_weight,
        row(recur_bias),
        input_weight,
        row(input_bias),
        row(rate),
    )


def shift(values, axis, count, step):
    return lax.ppermute(values, axis, [(i, (i + step) % count) for i in range(count)])


def take(values, index, size, axis=0):
    return lax.dynamic_slice_in_dim(values, index * size, size, axis)


def pair_gather(weight, count, axis):
    groups = [list(range(parity, count, 2)) for parity in range(2)]
    own = lax.all_gather(weight, "fs", axis=axis, axis_index_groups=groups, tiled=True)
    other = lax.ppermute(own, "fs", [(i, i ^ 1) for i in range(count)])
    return own, other


def pair_columns(values, count, parity):
    rows, width = values.shape
    size = width // count
    blocks = [values[:, i * size : (i + 1) * size] for i in range(count)]
    even = jnp.concatenate(blocks[0::2], axis=1)
    odd = jnp.concatenate(blocks[1::2], axis=1)
    return jnp.where(parity == 0, even, odd), jnp.where(parity == 0, odd, even)


def scatter_rows(partial, n_tp, me):
    size = partial.shape[0] // n_tp
    total = take(partial, me, size).astype(jnp.float32)
    for step in range(1, n_tp):
        sent = take(partial, lax.rem(me + step, n_tp), size)
        total = total + shift(sent, "tp", n_tp, step).astype(jnp.float32)
    return total


def collect_rows(share, n_tp, me):
    size = share.shape[0]
    if n_tp == 2:
        other = shift(share, "tp", n_tp, 1)
        first = jnp.where(me == 0, share, other)
        second = jnp.where(me == 0, other, share)
        return jnp.concatenate([first, second], axis=0)
    whole = jnp.zeros((size * n_tp, share.shape[1]), share.dtype)
    whole = lax.dynamic_update_slice_in_dim(whole, share, me * size, 0)
    for step in range(1, n_tp):
        got = shift(share, "tp", n_tp, step)
        whole = lax.dynamic_update_slice_in_dim(whole, got, lax.rem(me - step + n_tp, n_tp) * size, 0)
    return whole


def plain(
    n_rep,
    n_fs,
    n_tp,
    tokens,
    mixer_gain,
    mix_weight,
    mixer_conv,
    mixer_offset,
    recur_weight,
    recur_bias,
    input_weight,
    input_bias,
    decay_logit,
    out_weight,
    channel_gain,
    gate_weight,
    up_weight,
    gate_conv,
    gate_offset,
    down_weight,
):
    rep = lax.axis_index("rep")
    tp = lax.axis_index("tp")
    parity = lax.rem(lax.axis_index("fs"), 2)
    length = tokens.shape[0]
    units = gate_weight.shape[1] // n_rep

    both = jnp.concatenate([mix_weight, out_weight.T], axis=1)
    both_full = lax.all_gather(both, "fs", axis=0, tiled=True)
    channels = mix_weight.shape[1]
    mixer_full, out_full = both_full[:, :channels], both_full[:, channels:]
    gate_own, gate_other = pair_gather(take(gate_weight, rep, units, 1), n_fs, 0)
    up_own, up_other = pair_gather(take(up_weight, rep, units, 1), n_fs, 0)
    down_full = lax.all_gather(take(down_weight, rep, units, 0), "fs", axis=1, tiled=True)
    gate_taps = take(gate_conv, rep, units, 1)
    gate_base = take(gate_offset, rep, units, 0)

    normed = rms_rows(tokens, mixer_gain)
    branch = jnp.dot(normed, mixer_full, preferred_element_type=jnp.float32).astype(jnp.bfloat16)
    recurrent = mixer(
        branch,
        mixer_conv,
        mixer_offset,
        recur_weight,
        recur_bias,
        input_weight,
        input_bias,
        lru_scale * jax.nn.log_sigmoid(decay_logit),
    )
    mixer_term = lax.dot_general(
        recurrent, out_full, (((1,), (1,)), ((), ())), preferred_element_type=jnp.float32
    )
    mixer_share = scatter_rows(mixer_term.astype(jnp.bfloat16), n_tp, tp)
    rows = length // n_tp
    residual = (take(tokens, tp, rows).astype(jnp.float32) + mixer_share).astype(jnp.bfloat16)
    normed_share = rms_rows(residual, channel_gain)

    shares = [normed_share]
    for step in range(1, n_rep):
        shares.append(shift(normed_share, "rep", n_rep, step))

    def channel_mixer(share):
        rows_in = collect_rows(share, n_tp, tp)
        left, right = pair_columns(rows_in, n_fs, parity)
        gate_rows = jnp.dot(left, gate_own, preferred_element_type=jnp.float32)
        gate_rows = gate_rows + jnp.dot(right, gate_other, preferred_element_type=jnp.float32)
        up_rows = jnp.dot(left, up_own, preferred_element_type=jnp.float32)
        up_rows = up_rows + jnp.dot(right, up_other, preferred_element_type=jnp.float32)
        gate_rows = gate_rows.astype(jnp.bfloat16)
        up_rows = up_rows.astype(jnp.bfloat16)
        gate_mixed = causal_conv(gate_rows.astype(jnp.float32), gate_taps, gate_base)
        hidden = (jax.nn.gelu(gate_mixed) * up_rows.astype(jnp.float32)).astype(jnp.bfloat16)
        return jnp.dot(hidden, down_full, preferred_element_type=jnp.float32).astype(jnp.bfloat16)

    own_terms = channel_mixer(shares[0])
    total = None
    for step in range(1, n_rep):
        summed = scatter_rows(channel_mixer(shares[step]), n_tp, tp).astype(jnp.bfloat16)
        back = shift(summed, "rep", n_rep, -step).astype(jnp.float32)
        total = back if total is None else total + back
    own = scatter_rows(own_terms, n_tp, tp)
    total = own if total is None else own + total
    result = (residual.astype(jnp.float32) + total).astype(jnp.bfloat16)
    return collect_rows(result, n_tp, tp)


MESH = pl.DeviceIdType.MESH
unit_tile = 256
pieces = 2


class Copies:
    def __init__(self, send_sem, is_mid):
        self.send_sem = send_sem
        self.conds = {"all": None, "mid": is_mid, "end": jnp.logical_not(is_mid)}
        self.sizes = [{"all": 0, "mid": 0, "end": 0} for _ in range(send_sem.shape[0])]

    def send(self, src, dst, recv_sem, device, group, kind="all", now=None):
        def start():
            copy = pltpu.make_async_remote_copy(
                src_ref=src(),
                dst_ref=dst(),
                send_sem=self.send_sem.at[group],
                recv_sem=recv_sem(),
                device_id=device,
                device_id_type=MESH,
            )
            copy.start()

        self.sizes[group][kind] += size_of(src())
        guarded(both_of(self.conds[kind], now), start)

    def drain(self, spans, device):
        for group, size in enumerate(self.sizes):
            for kind in ("all",) if size["mid"] == size["end"] else ("mid", "end"):
                total = size["all"] + size["mid" if kind == "all" else kind]

                def wait(total=total, group=group):
                    wait_sent(span_of(spans, total), self.send_sem.at[group], device)

                guarded(self.conds[kind], wait)


def size_of(ref):
    return math.prod(ref.shape) * 2


def span_of(spans, total):
    for ref in spans:
        count, rows, columns = ref.shape
        need = total // (2 * columns)
        lots = -(-need // rows)
        if lots <= count and need % lots == 0:
            return ref.at[pl.ds(0, lots), pl.ds(0, need // lots), :]
    raise ValueError("no span")


def wait_sent(ref, sem, device):
    pltpu.make_async_remote_copy(
        src_ref=ref, dst_ref=ref, send_sem=sem, recv_sem=sem, device_id=device, device_id_type=MESH
    ).wait_send()


def guarded(cond, act):
    if cond is None:
        act()
    else:
        pl.when(cond)(lambda: act())


def both_of(first, second):
    if first is None or second is None:
        return second if first is None else first
    return jnp.logical_and(first, second)


def rows_at(start, size):
    if isinstance(start, int):
        return pl.ds(start, size)
    return pl.ds(pl.multiple_of(start, size), size)


def layer_kernel(
    n_z,
    tokens,
    mixer_gain,
    mix_w,
    taps,
    offset,
    recur_w,
    recur_b,
    input_w,
    input_b,
    logit,
    out_w,
    channel_gain,
    gate_w,
    up_w,
    gate_taps,
    gate_base,
    down_w,
    out,
    tok,
    mixb,
    outb,
    branch,
    recurrent,
    term_send,
    term_recv,
    term_own,
    residual,
    acts,
    gub,
    gub_swap,
    dnb,
    dnb_swap,
    hid,
    half_send,
    half_recv,
    half_own,
    chip_own,
    chip_send,
    chip_recv,
    local_sem,
    send_sem,
    mix_sem,
    gu_sem,
    dn_sem,
    term_sem,
    act_sem,
    half_send_sem,
    half_recv_sem,
    chip_send_sem,
    chip_recv_sem,
    out_send_sem,
    out_recv_sem,
):
    x = lax.axis_index("rep")
    f = lax.axis_index("fs")
    t = lax.axis_index("tp")
    z, y = f // 2, f % 2
    n_f = 2 * n_z
    length, width = tokens.shape
    depth, channels = mix_w.shape
    chunks = gub.shape[0]
    units = chunks * unit_tile
    half = length // 2
    dim = recur_w.shape[1]

    def at(x_at, z_at, y_at, t_at):
        return (x_at, z_at * 2 + y_at, t_at)

    other_x, other_y, other_t = 1 - x, 1 - y, 1 - t
    near = {1: at(other_x, z, y, t), 2: at(x, z, other_y, t), 3: at(other_x, z, other_y, t)}
    partner = at(x, z, y, other_t)
    beside = z * 2 + other_y
    toward = jnp.where(2 * z < n_z, 1, n_z - 1)
    column = [(z + step * toward) % n_z for step in range(n_z)]
    edge = n_z - 1
    is_mid = jnp.logical_and(z > 0, z < edge)
    mid_from = column[1:3]
    mid_to = column[edge]
    mid_device = at(x, mid_to, y, t)

    def relayed(z_at):
        return jnp.logical_and(is_mid, z_at != mid_to)

    def direct(step):
        return ("all", "end", "mid")[step - 1]

    barrier = pltpu.get_barrier_semaphore()

    def greet(peer):
        pl.semaphore_signal(barrier, inc=1, device_id=peer, device_id_type=MESH)

    beside_peers = [near[1], near[2], near[3], partner]
    for peer in [at(x, column[1], y, t)] + beside_peers:
        greet(peer)
    for step in range(2, n_z):
        guarded(is_mid, functools.partial(greet, at(x, column[step], y, t)))

    quarter = x * 2 + y
    quarter_swap = x * 2 + other_y
    numbers = itertools.count()

    def bring(whole, *pairs):
        sem = local_sem.at[next(numbers)]
        for src, dst in pairs:
            pltpu.make_async_copy(src, dst, sem).start()
        return pltpu.make_async_copy(whole, whole, sem)

    own_rows = rows_at(f * depth, depth)
    both_blocks = mixb.at[pl.ds(0, 2 * depth), :]
    got_mix = bring(both_blocks, (mix_w, mixb.at[own_rows, :]), (out_w, outb.at[:, own_rows]))

    def unit_cols(which, chunk):
        return rows_at(which * units + chunk * unit_tile, unit_tile)

    low, high = pl.ds(0, unit_tile), pl.ds(unit_tile, unit_tile)
    got_own, got_swap = [], []
    for c in range(chunks):
        got_own.append(
            bring(
                gub.at[c, own_rows, :],
                (gate_w.at[:, unit_cols(quarter, c)], gub.at[c, own_rows, low]),
                (up_w.at[:, unit_cols(quarter, c)], gub.at[c, own_rows, high]),
            )
        )
        got_swap.append(
            bring(
                gub_swap.at[c],
                (gate_w.at[:, unit_cols(quarter_swap, c)], gub_swap.at[c, :, low]),
                (up_w.at[:, unit_cols(quarter_swap, c)], gub_swap.at[c, :, high]),
            )
        )
    got_tok = bring(tok, (tokens, tok))
    got_own.append(bring(dnb.at[f], (down_w.at[rows_at(quarter * units, units), :], dnb.at[f])))
    got_swap.append(bring(dnb_swap, (down_w.at[rows_at(quarter_swap * units, units), :], dnb_swap)))

    pl.semaphore_wait(barrier, len(beside_peers) + 2)

    copies = Copies(send_sem, is_mid)
    mix_group, swap_group, down_group, act_group = range(chunks, chunks + 4)

    def arrived(dst, sem, cond=None):
        def wait():
            copy = pltpu.make_async_remote_copy(
                src_ref=dst(),
                dst_ref=dst(),
                send_sem=sem(),
                recv_sem=sem(),
                device_id=partner,
                device_id_type=MESH,
            )
            copy.wait_recv()

        guarded(cond, wait)

    part_rows, part_out = depth // 2, channels // 2

    def mix_pieces(block, part):
        return [
            (
                lambda: mixb.at[rows_at(block * depth + part * part_rows, part_rows), :],
                lambda: mix_sem.at[block, part],
            ),
            (
                lambda: outb.at[rows_at(part * part_out, part_out), rows_at(block * depth, depth)],
                lambda: mix_sem.at[block, part],
            ),
        ]

    def send_mix(block, part, device, kind="all"):
        for ref, sem in mix_pieces(block, part):
            copies.send(ref, ref, sem, device, mix_group, kind)

    def wait_mix(block, part):
        arrived(lambda: mixb.at[rows_at(block * depth, depth), :], lambda: mix_sem.at[block, part])

    def weight_ref(stage, block):
        if stage == chunks:
            return lambda: dnb.at[block], lambda: dn_sem.at[block, 0]
        return lambda: gub.at[stage, rows_at(block * depth, depth), :], lambda: gu_sem.at[stage, block]

    def send_swap(stage):
        got_swap[stage].wait()
        ref, sem = weight_ref(stage, f)
        copies.send(lambda: dnb_swap if stage == chunks else gub_swap.at[stage], ref, sem, near[2], swap_group)

    def send_block(stage, block, steps=range(1, n_z), kind=None):
        ref, sem = weight_ref(stage, block)
        for step in steps:
            copies.send(ref, ref, sem, at(x, column[step], y, t), stage, kind or direct(step))

    def send_own(stage):
        got_own[stage].wait()
        send_block(stage, f)

    def send_first(inner):
        if not inner:
            got_own[0].wait()
            send_block(0, f, range(2, n_z))
        send_block(0, f, range(1, 2), "mid" if inner else "end")

    def send_beside(stage):
        arrived(*weight_ref(stage, beside))
        send_block(stage, beside)

    piece_width = depth // pieces

    def down_ref(block, piece):
        cols = rows_at(piece * piece_width, piece_width)
        return lambda: dnb.at[block, :, cols], lambda: dn_sem.at[block, piece]

    def send_down():
        got_own[chunks].wait()
        arrived(*weight_ref(chunks, beside))
        for side in range(2):
            for piece in range(pieces):
                ref, sem = down_ref(z * 2 + side, piece)
                for step in range(1, n_z):
                    copies.send(ref, ref, sem, at(x, column[step], y, t), down_group, direct(step))

    side_blocks = [[z_at * 2 + side for z_at in mid_from] for side in (y, other_y)]
    mid_blocks = [[z_at * 2 + side for side in range(2)] for z_at in mid_from]

    def relay_ref(ref, sem, group, now):
        arrived(ref, sem, both_of(is_mid, now))
        copies.send(ref, ref, sem, mid_device, group, "mid", now)

    def relay_blocks(stage, blocks, now=None):
        for block in blocks:
            relay_ref(*weight_ref(stage, block), stage, now)

    def relay_down(blocks, now=None):
        for block in blocks:
            for piece in range(pieces):
                relay_ref(*down_ref(block, piece), down_group, now)

    def wait_stage(stage, now=None):
        for step in range(1, n_z):
            for side in (y, other_y):
                ref, sem = weight_ref(stage, column[step] * 2 + side)
                fresh = jnp.logical_not(is_mid) if step < edge else None
                arrived(ref, sem, both_of(fresh, now))

    got_mix.wait()
    for step in range(1, n_z):
        send_mix(f, x, at(x, column[step], y, t), direct(step))
    for part in range(2):
        send_mix(f, part, near[2])
    send_first(False)
    send_swap(0)

    def norm_rows(source, gain, dest, total, size=64):
        def body(i, carry):
            at_rows = rows_at(i * size, size)
            widened = source[at_rows, :].astype(jnp.float32)
            scaled = widened * lax.rsqrt(jnp.mean(widened * widened, axis=-1, keepdims=True) + epsilon)
            dest[at_rows, :] = (scaled * gain[...]).astype(jnp.bfloat16)
            return carry

        lax.fori_loop(0, total // size, body, 0)

    got_tok.wait()
    norm_rows(tok, mixer_gain, acts.at[0], length)

    order = range(1, n_z)
    for step in order:
        block = column[step] * 2 + y
        wait_mix(block, x)
        send_mix(block, x, near[2])
        send_mix(block, x, near[1])
        if step < edge:
            send_mix(block, x, mid_device, "mid")
    send_first(True)
    for stage in range(1, chunks + 1):
        send_swap(stage)
    send_beside(0)
    relay_blocks(0, side_blocks[0])
    send_own(1)
    for step in order:
        block = column[step] * 2 + other_y
        wait_mix(block, x)
        send_mix(block, x, near[1])
    relay_blocks(0, side_blocks[1])
    send_beside(1)
    for part in range(2):
        wait_mix(beside, part)
    for step in order:
        for side in (y, other_y):
            wait_mix(column[step] * 2 + side, other_x)
    def branch_body(j, carry):
        cols = rows_at(j * 256, 256)
        branch[:, cols] = (
            jnp.dot(acts[0], mixb[:, cols], preferred_element_type=jnp.float32).astype(jnp.bfloat16).astype(jnp.float32)
        )
        return carry

    lax.fori_loop(0, channels // 256, branch_body, 0)

    def block_body(k, carry):
        cols = rows_at(k * dim, dim)
        recurrent[:, cols] = recur_block(
            branch[:, cols],
            taps[:, cols],
            offset[:, cols],
            recur_w[k],
            recur_b[:, cols],
            input_w[k],
            input_b[:, cols],
            lru_scale * log_sigmoid(logit[:, cols]),
        )
        return carry

    lax.fori_loop(0, channels // dim, block_body, 0)

    relay_blocks(1, side_blocks[0])
    send_own(2)
    send_beside(2)

    def project(which, dest):
        rows = rows_at(which * half, half)

        def body(j, carry):
            cols = rows_at(j * 512, 512)
            dest[:, cols] = jnp.dot(recurrent[rows, :], outb[:, cols], preferred_element_type=jnp.float32).astype(
                jnp.bfloat16
            )
            return carry

        lax.fori_loop(0, width // 512, body, 0)

    project(other_t, term_send)
    copies.send(lambda: term_send, lambda: term_recv, lambda: term_sem.at[0], partner, act_group)
    project(t, term_own)
    arrived(lambda: term_recv, lambda: term_sem.at[0])
    mine = rows_at(t * half, half)
    theirs = rows_at(other_t * half, half)

    def residual_body(i, carry):
        rows = rows_at(i * 64, 64)
        total = term_own[rows, :].astype(jnp.float32) + term_recv[rows, :].astype(jnp.float32)
        base = tok[rows_at(t * half + i * 64, 64), :].astype(jnp.float32)
        residual[rows, :] = (base + total).astype(jnp.bfloat16)
        return carry

    lax.fori_loop(0, half // 64, residual_body, 0)
    norm_rows(residual, channel_gain, acts.at[0, mine, :], half)
    def act_part(slot, rows):
        return lambda: acts.at[slot, rows, :]

    def act_arrival(slot, hop):
        return lambda: act_sem.at[slot, hop]

    for slot in (1, 2, 3):
        copies.send(act_part(0, mine), act_part(slot, mine), act_arrival(slot, 0), near[slot], act_group)
    copies.send(act_part(0, mine), act_part(0, mine), act_arrival(0, 1), partner, act_group)
    relay_blocks(1, side_blocks[1])
    relay_blocks(2, side_blocks[0])
    relay_blocks(2, side_blocks[1])
    send_down()

    def pass_on(slot, now):
        arrived(act_part(slot, mine), act_arrival(slot, 0), now)
        copies.send(act_part(slot, mine), act_part(slot, mine), act_arrival(slot, 1), partner, act_group, now=now)

    def wait_acts(slot, now):
        arrived(act_part(slot, theirs), act_arrival(slot, 1), now)

    early = max(chunks - 1, 1)
    plan = [(slot, c) for slot in range(4) for c in range(early)]
    plan += [(slot, c) for c in range(early, chunks) for slot in range(4)]
    hooks = [[] for _ in plan]
    for number, (slot, c) in enumerate(plan):
        if slot == 0:
            hooks[number].append(functools.partial(wait_stage, c))
        if c == 0:
            hooks[number].append(functools.partial(wait_acts, slot))
    for slot in (1, 2, 3):
        hooks[slot * early - 1].append(functools.partial(pass_on, slot))

    rows_iota = lax.broadcasted_iota(jnp.int32, (length, unit_tile), 0)

    def gate_body(number, carry):
        late = number >= 4 * early
        slot = jnp.where(late, (number - 4 * early) % 4, number // early)
        c = jnp.where(late, early + (number - 4 * early) // 4, number % early)
        for index, acting in enumerate(hooks):
            for act in acting:
                act(now=number == index)

        both = jnp.dot(acts[slot], gub[c], preferred_element_type=jnp.float32)
        gate = both[:, :unit_tile].astype(jnp.bfloat16).astype(jnp.float32)
        up = both[:, unit_tile:].astype(jnp.bfloat16).astype(jnp.float32)
        cols = rows_at(quarter * units + c * unit_tile, unit_tile)
        width_taps = gate_taps.shape[0]
        mixed = gate_base[:, cols] + gate * gate_taps[width_taps - 1 : width_taps, cols]
        for back in range(1, width_taps):
            moved = jnp.where(rows_iota >= back, pltpu.roll(gate, back, 0), 0.0)
            mixed = mixed + moved * gate_taps[width_taps - 1 - back : width_taps - back, cols]
        hidden = (jax.nn.gelu(mixed) * up).astype(jnp.bfloat16)
        place = rows_at(c * unit_tile, unit_tile)
        rows = rows_at(slot * half, half)
        hid[0, rows, place] = hidden[:half]
        hid[1, rows, place] = hidden[half:]
        return carry

    lax.fori_loop(0, len(plan), gate_body, 0)
    relay_down(mid_blocks[0])

    n_b = n_f * pieces

    def block_of(i):
        k, side = i // (2 * pieces), (i // pieces) % 2
        return (((z // 2 + k // 2) % 2) * 2 + (z % 2 + k % 2) % 2) * 2 + side

    def cols_of(i):
        return rows_at((block_of(i) * pieces + i % pieces) * piece_width, piece_width)

    def half_copy(i):
        return pltpu.make_async_remote_copy(
            src_ref=half_send.at[i],
            dst_ref=half_recv.at[i],
            send_sem=half_send_sem.at[0],
            recv_sem=half_recv_sem.at[i],
            device_id=partner,
            device_id_type=MESH,
        )

    def chip_copy(i, slot):
        return pltpu.make_async_remote_copy(
            src_ref=chip_send.at[i, slot - 1],
            dst_ref=chip_recv.at[i, slot - 1],
            send_sem=chip_send_sem.at[0],
            recv_sem=chip_recv_sem.at[i],
            device_id=near[slot],
            device_id_type=MESH,
        )

    def out_copy(i):
        return pltpu.make_async_remote_copy(
            src_ref=out.at[mine, cols_of(i)],
            dst_ref=out.at[mine, cols_of(i)],
            send_sem=out_send_sem.at[0],
            recv_sem=out_recv_sem.at[0],
            device_id=partner,
            device_id_type=MESH,
        )

    lag = 3

    def down_body(i, carry):
        relay_down(mid_blocks[1], i == 2 * pieces)

        block, cols = block_of(i), rows_at((i % pieces) * piece_width, piece_width)
        fresh = jnp.logical_and(block != f, block != beside)
        fresh = jnp.logical_and(fresh, jnp.logical_not(relayed(block // 2)))
        arrived(lambda: dnb.at[block, :, cols], lambda: dn_sem.at[block, i % pieces], fresh)
        weight = dnb[block, :, cols]
        half_send[i] = jnp.dot(hid[other_t], weight, preferred_element_type=jnp.float32).astype(jnp.bfloat16)
        half_copy(i).start()
        half_own[...] = jnp.dot(hid[t], weight, preferred_element_type=jnp.float32).astype(jnp.bfloat16)
        half_copy(i).wait_recv()

        def add(slot):
            rows = pl.ds(slot * half, half)
            return half_own[rows, :].astype(jnp.float32) + half_recv[i, rows, :].astype(jnp.float32)

        before = None
        for slot in (3, 1, 2):
            chip_send[i, slot - 1] = add(slot).astype(jnp.bfloat16)
            if before is not None:
                chip_copy(i, before).start()
            before = slot
        chip_own[i] = add(0)
        chip_copy(i, before).start()

        pl.when(i >= lag)(lambda: finish(i - lag))
        return carry

    def finish(m):
        arrived(lambda: chip_recv.at[m], lambda: chip_recv_sem.at[m])
        total = chip_own[m]
        for slot in range(3):
            total = total + chip_recv[m, slot].astype(jnp.float32)
        out[mine, cols_of(m)] = (residual[:, cols_of(m)].astype(jnp.float32) + total).astype(jnp.bfloat16)
        out_copy(m).start()

    def finish_body(m, carry):
        finish(m)
        return carry

    lax.fori_loop(0, n_b, down_body, 0)
    copies.drain((gub, acts), partner)
    lax.fori_loop(n_b - lag, n_b, finish_body, 0)

    wait_sent(half_send, half_send_sem.at[0], partner)
    wait_sent(chip_send, chip_send_sem.at[0], partner)
    wait_sent(out.at[mine, :], out_send_sem.at[0], partner)
    arrived(lambda: out.at[theirs, :], lambda: out_recv_sem.at[0])


def log_sigmoid(v):
    small = jnp.exp(-jnp.abs(v))
    ratio = small / (2.0 + small)
    square = ratio * ratio
    series = 1.0 / 15.0
    for order in (13.0, 11.0, 9.0, 7.0, 5.0, 3.0, 1.0):
        series = 1.0 / order + square * series
    return jnp.minimum(v, 0.0) - 2.0 * ratio * series


def recur_block(branch, taps, offset, recur_weight, recur_bias, input_weight, input_bias, rate):
    length = branch.shape[0]
    width = taps.shape[0]
    rows = lax.broadcasted_iota(jnp.int32, branch.shape, 0)

    def shifted(values, step, fill):
        return jnp.where(rows >= step, pltpu.roll(values, step, 0), fill)

    total = offset + branch * taps[width - 1 : width, :]
    for back in range(1, width):
        total = total + shifted(branch, back, 0.0) * taps[width - 1 - back : width - back, :]
    smoothed = total.astype(jnp.bfloat16)
    recur = jnp.dot(smoothed, recur_weight, preferred_element_type=jnp.float32)
    recur_gate = jax.nn.sigmoid(recur + recur_bias)
    gated = jnp.dot(smoothed, input_weight, preferred_element_type=jnp.float32)
    input_gate = jax.nn.sigmoid(gated + input_bias)
    log_decay = recur_gate * rate
    state = jnp.sqrt(one_minus_exp(2.0 * log_decay)) * (input_gate * smoothed.astype(jnp.float32))
    decay = jnp.exp(log_decay)
    step = 1
    while step < length:
        state = state + decay * shifted(state, step, 0.0)
        if 2 * step < length:
            decay = decay * shifted(decay, step, 1.0)
        step *= 2
    return state.astype(jnp.bfloat16)


def fused(
    n_fs,
    tokens,
    mixer_gain,
    mix_weight,
    mixer_conv,
    mixer_offset,
    recur_weight,
    recur_bias,
    input_weight,
    input_bias,
    decay_logit,
    out_weight,
    channel_gain,
    gate_weight,
    up_weight,
    gate_conv,
    gate_offset,
    down_weight,
):
    n_z = n_fs // 2
    length, width = tokens.shape
    depth, channels = mix_weight.shape
    units = gate_weight.shape[1] // 4
    chunks = units // unit_tile
    half = length // 2
    n_b = n_fs * pieces
    row = lambda v: v.reshape(1, v.shape[0])
    hbm = pl.BlockSpec(memory_space=pl.ANY)
    vmem = pl.BlockSpec(memory_space=pltpu.VMEM)
    bf16, f32 = jnp.bfloat16, jnp.float32
    dma = pltpu.SemaphoreType.DMA
    rows_out = pl.pallas_call(
        functools.partial(layer_kernel, n_z),
        name="layer",
        in_specs=[hbm, vmem, hbm] + [vmem] * 7 + [hbm, vmem, hbm, hbm, vmem, vmem, hbm],
        out_specs=vmem,
        out_shape=pltpu.VMEM((length, width), bf16),
        scratch_shapes=[
            pltpu.VMEM((length, width), bf16),
            pltpu.VMEM((width, channels), bf16),
            pltpu.VMEM((channels, width), bf16),
            pltpu.VMEM((length, channels), f32),
            pltpu.VMEM((length, channels), bf16),
            pltpu.VMEM((half, width), bf16),
            pltpu.VMEM((half, width), bf16),
            pltpu.VMEM((half, width), bf16),
            pltpu.VMEM((half, width), bf16),
            pltpu.VMEM((4, length, width), bf16),
            pltpu.VMEM((chunks, width, 2 * unit_tile), bf16),
            pltpu.VMEM((chunks, depth, 2 * unit_tile), bf16),
            pltpu.VMEM((n_fs, units, depth), bf16),
            pltpu.VMEM((units, depth), bf16),
            pltpu.VMEM((2, 4 * half, units), bf16),
            pltpu.VMEM((n_b, 4 * half, depth // pieces), bf16),
            pltpu.VMEM((n_b, 4 * half, depth // pieces), bf16),
            pltpu.VMEM((4 * half, depth // pieces), bf16),
            pltpu.VMEM((n_b, half, depth // pieces), f32),
            pltpu.VMEM((n_b, 3, half, depth // pieces), bf16),
            pltpu.VMEM((n_b, 3, half, depth // pieces), bf16),
            dma((4 + 2 * chunks,)),
            dma((chunks + 4,)),
            dma((n_fs, 2)),
            dma((chunks, n_fs)),
            dma((n_fs, pieces)),
            dma((1,)),
            dma((4, 2)),
            dma((1,)),
            dma((n_b,)),
            dma((1,)),
            dma((n_b,)),
            dma((1,)),
            dma((1,)),
        ],
        compiler_params=pltpu.CompilerParams(
            collective_id=0, has_side_effects=True, vmem_limit_bytes=56 * 2**20
        ),
    )(
        tokens,
        row(mixer_gain),
        mix_weight,
        mixer_conv,
        row(mixer_offset),
        recur_weight,
        row(recur_bias),
        input_weight,
        row(input_bias),
        row(decay_logit),
        out_weight,
        row(channel_gain),
        gate_weight,
        up_weight,
        gate_conv,
        row(gate_offset),
        down_weight,
    )
    return rows_out


def local(n_rep, n_fs, n_tp, *arrays):
    units, columns = arrays[16].shape
    fits = n_rep == 2 and n_tp == 2 and n_fs == 8
    if fits and units == 12 * unit_tile and columns % 128 == 0:
        return fused(n_fs, *arrays)
    return plain(n_rep, n_fs, n_tp, *arrays)


def solution(mesh):
    in_specs = (
        P(("rep", "fs"), None),
        P(),
        P("fs", "tp"),
        P(None, "tp"),
        P("tp"),
        P("tp", None, None),
        P("tp"),
        P("tp", None, None),
        P("tp"),
        P("tp"),
        P("tp", "fs"),
        P(),
        P("fs", "tp"),
        P("fs", "tp"),
        P(None, "tp"),
        P("tp"),
        P("tp", "fs"),
    )
    out_specs = P(("rep", "fs"), None)
    body = functools.partial(local, mesh.shape["rep"], mesh.shape["fs"], mesh.shape["tp"])
    return jax.shard_map(body, mesh=mesh, in_specs=in_specs, out_specs=out_specs, check_vma=False)
```
